256 devices in a mesh: ep: 64 (over z, y, core), tp: 4 (over x).
Axes of the slice: x: 4, y: 4, z: 8, core: 2. Of those that a mesh axis runs over, the one named last changes fastest.
Arguments:
- mixer_in: bfloat16 [32768, 2048], P('ep'), may hold values from -6 to 6
- mixer_gain: float32 [2048], replicated, may hold values from 0.1 to 1.9
- query_weight: bfloat16 [2048, 1024], P(None, 'tp'), may hold values from -0.125 to 0.125
- key_weight: bfloat16 [2048, 1024], P(None, 'tp'), may hold values from -0.125 to 0.125
- value_weight: bfloat16 [2048, 1024], P(None, 'tp'), may hold values from -0.125 to 0.125
- input_gate: float32 [8, 32768], P('tp', 'ep'), may hold values from -4 to 240
- forget_gate: float32 [8, 32768], P('tp', 'ep'), may hold values from 0 to 25
- head_gain: float32 [1024], replicated, may hold values from 0.1 to 1.9
- mixer_out_weight: bfloat16 [1024, 2048], P('tp'), may hold values from -0.1875 to 0.1875
- expert_in: bfloat16 [16384, 2048], P('ep'), may hold values from -6 to 6
- expert_gain: float32 [2048], replicated, may hold values from 0.1 to 1.9
- group_router: bfloat16 [2048, 16], replicated, may hold values from -0.125 to 0.125
- expert_router: bfloat16 [2048, 64], replicated, may hold values from -0.125 to 0.125
- routes: int32 [16384, 2], P('ep'), may hold values from 0 to 63, all different within a row; in each aligned block of 256 rows (0 to 255, 256 to 511, ...) at most 16 rows name the same one
- gate_experts: bfloat16 [64, 2048, 1024], P('ep', None, 'tp'), may hold values from -0.125 to 0.125
- up_experts: bfloat16 [64, 2048, 1024], P('ep', None, 'tp'), may hold values from -0.125 to 0.125
- down_experts: bfloat16 [64, 1024, 2048], P('ep', 'tp'), may hold values from -0.1875 to 0.1875
Outputs:
- mixer_out: bfloat16 [32768, 2048], P(('ep', 'tp'))
- expert_out: bfloat16 [16384, 2048], P('ep', 'tp')
The draws below stay inside these ranges and needn't reach their ends.
Inputs may be any that keep to these rules, and one draw needn't show every extreme that they name: `routes`: each row names 2 different experts. In each aligned block of 256 rows (the rows of one index of ep) no expert is named by more than 16 rows, a bound that some block reaches.
All inputs are finite; a program needn't handle non-finite values.
Results may differ from the reference program's by a relative error of at most 0.014.
The reference program's roundings to bfloat16 on the way count: a program that leaves them out, or rounds other values in their place, can miss the bound.
Values may be sent and summed in bfloat16 or wider, within the bound.
No kernel may reach another device: no remote copies, remote signals or barrier semaphores. Data moves between devices by JAX's collectives and lax.ppermute only.
A program may use at most 128 MiB of HBM per device.

```python
import math
import jax
import jax.numpy as jnp
import numpy as np
from jax import lax

D = 2048
HEADS = 8
W = 1024
FF = 1024
BLOCK = 128
TOPK = 2
TA_DEV = 512
TB_DEV = 256
SEQUENCE_SPAN = 32768
TB = 16384
EXPERTS = 64
GROUPS = 16
CAP = 16
N_EP = 64
N_TP = 4


def draw_input_gate(key, part):
    value_rows = jnp.clip(jax.random.normal(jax.random.fold_in(key, 11), (HEADS, SEQUENCE_SPAN), jnp.float32), -4.0, 4.0)
    return value_rows


def draw_forget_gate(key, part):
    sequence_place = jnp.arange(SEQUENCE_SPAN)
    fast_cut = 5
    is_fast = jax.random.randint(jax.random.fold_in(key, 21), (HEADS,), 0, 10) < fast_cut
    factors = jnp.exp(jax.random.uniform(jax.random.fold_in(key, 22), (SEQUENCE_SPAN // TA_DEV,), jnp.float32, math.log(0.4), math.log(2.5)))
    noise = jnp.exp(0.7 * jnp.clip(jax.random.normal(jax.random.fold_in(key, 23), (HEADS, SEQUENCE_SPAN), jnp.float32), -4.0, 4.0))
    slow_rate = 0.3 / SEQUENCE_SPAN * factors[sequence_place // TA_DEV]
    rate = jnp.where(is_fast[:, None], 1.0 / 40.0, slow_rate[None, :]) * noise
    value_rows = -jnp.log(rate)
    spike_location = jax.random.randint(jax.random.fold_in(key, 25), (3,), 0, SEQUENCE_SPAN)
    retain_flag = jax.random.uniform(jax.random.fold_in(key, 26), (HEADS, 3), jnp.float32, 0.5, 0.8)
    spike_magnitude = jnp.log(retain_flag / (1.0 - retain_flag))
    for column_slot in range(3):
        value_rows = jnp.where(sequence_place[None, :] == spike_location[column_slot], spike_magnitude[:, column_slot:column_slot + 1], value_rows)
    return value_rows


def steps_of(rng, extent, shards, smallest, largest):
    level, own = 1.0, jax.random.fold_in(rng, 6)
    for dim, parts in shards:
        heights = jnp.exp(jax.random.uniform(jax.random.fold_in(own, dim), (parts,), jnp.float32, smallest / len(shards), largest / len(shards)))
        level = level * jnp.repeat(heights, extent[dim] // parts).reshape([-1 if axis == dim else 1 for axis in range(len(extent))])
    return level


def routed_block(key, own, number, rows, count, top, limit, skew):
    ranking = jax.random.permutation(key, count)
    crowded, common = shares(count, rows * top, limit, skew, True), shares(count, rows * top, limit, skew, False)
    places = jnp.arange(count)

    def named(lengths, offset_by):
        used = int((lengths > 0).sum())
        fixed = max(1, used // 4)
        shifted = fixed + (places - fixed + offset_by * (used - fixed)) % max(1, count - fixed)
        return jnp.zeros((count,), jnp.int32).at[ranking[jnp.where(places < fixed, places, shifted)]].set(jnp.asarray(lengths, jnp.int32))

    lengths = jnp.where(number % 4 == 0, named(crowded, number // 4), named(common, number - number // 4 - 1))
    mixed = jax.random.permutation(jax.random.fold_in(own, 3), count)
    source_of, sink = mixed[0:count // 2 * 2:2], mixed[1:count // 2 * 2:2]
    margin = jnp.minimum(lengths[source_of] - 1, limit - lengths[sink]) // 2
    margin = jnp.where((source_of == ranking[0]) | (sink == ranking[0]) | (lengths[sink] == 0), 0, jnp.maximum(margin, 0))
    shifted = jax.random.randint(jax.random.fold_in(own, 4), (count // 2,), 0, 1 << 20) % (margin + 1)
    lengths = lengths.at[source_of].add(-shifted).at[sink].add(shifted)
    labels = jnp.searchsorted(jnp.cumsum(lengths), jnp.arange(rows * top), side="right").astype(jnp.int32)
    table = labels.reshape(top, rows).T
    table = table[jax.random.permutation(jax.random.fold_in(own, 1), rows)]
    offset_by = jax.random.randint(jax.random.fold_in(own, 2), (rows, 1), 0, top)
    return jnp.take_along_axis(table, (jnp.arange(top)[None, :] + offset_by) % top, axis=1)


def shares(count, total, limit, slope, full):
    weights = [(1 << 20) // math.isqrt(standing ** slope) + 1 for standing in range(1, count + 1)]
    largest = limit if full else min(limit, max(-(-total // count), total * weights[0] // sum(weights)))
    least = 1 if total - largest >= count - 1 else 0
    holding, surplus = [largest] + [least] * (count - 1), total - largest - least * (count - 1)
    while surplus > 0:
        candidates = [i for i in range(1, count) if holding[i] < largest] or [i for i in range(1, count) if holding[i] < limit]
        whole, budget = sum([weights[i] for i in candidates]), surplus
        for i in candidates:
            addition = min(limit - holding[i], max(1, budget * weights[i] // whole), surplus)
            holding[i] = holding[i] + addition
            surplus = surplus - addition
    return np.array(holding)


def normal_values(key, dims, scale, bound, pieces=(), kind=jnp.bfloat16):
    entries = jax.random.normal(key, dims, jnp.float32) * scale
    if len(pieces) > 0:
        entries = steps_of(key, dims, pieces, -0.22, 0.18) * entries
    return jnp.clip(entries, min=-bound, max=bound).astype(kind)


def setup_inputs(seed: int = 0) -> dict:
    key_list = jax.random.split(jax.random.key(seed), 18)
    mixer_in = normal_values(key_list[0], (SEQUENCE_SPAN, D), 1.0, 6.0, ((0, 64),))
    mixer_gain = jnp.clip(1.0 + 0.18 * jax.random.normal(key_list[1], (D,), jnp.float32), 0.1, 1.9)
    query_weight = normal_values(key_list[2], (D, W), D ** -0.5, 0.125, ((1, 4),))
    key_weight = normal_values(key_list[3], (D, W), D ** -0.5, 0.125, ((1, 4),))
    value_weight = normal_values(key_list[4], (D, W), D ** -0.5, 0.125, ((1, 4),))
    input_gate = draw_input_gate(jax.random.fold_in(key_list[17], 71), 0)
    forget_gate = draw_forget_gate(jax.random.fold_in(key_list[17], 71), 0)
    head_gain = jnp.clip(1.0 + 0.18 * jax.random.normal(key_list[7], (W,), jnp.float32), 0.1, 1.9)
    mixer_out_weight = normal_values(key_list[8], (W, D), W ** -0.5, 0.1875, ((0, 4),))
    expert_in = normal_values(key_list[9], (TB, D), 1.0, 6.0, ((0, 64),))
    expert_gain = jnp.clip(1.0 + 0.18 * jax.random.normal(key_list[10], (D,), jnp.float32), 0.1, 1.9)
    group_router = normal_values(key_list[11], (D, GROUPS), D ** -0.5, 0.125)
    expert_router = normal_values(key_list[12], (D, EXPERTS), D ** -0.5, 0.125)
    routes_keys = jax.random.split(jax.random.fold_in(key_list[13], 1), TB // TB_DEV)
    routes_turns = jax.random.permutation(jax.random.fold_in(key_list[13], 3), TB // TB_DEV)
    routes = jax.vmap(lambda own, number: routed_block(jax.random.fold_in(key_list[13], 2), own, number, TB_DEV, EXPERTS, TOPK, CAP, 1))(routes_keys, routes_turns).reshape((TB, TOPK))
    gate_experts = normal_values(key_list[14], (EXPERTS, D, FF), D ** -0.5, 0.125, ((0, 64), (2, 4)))
    up_experts = normal_values(key_list[15], (EXPERTS, D, FF), D ** -0.5, 0.125, ((0, 64), (2, 4)))
    down_experts = normal_values(key_list[16], (EXPERTS, FF, D), FF ** -0.5, 0.1875, ((0, 64), (1, 4)))
    return dict(mixer_in=mixer_in, mixer_gain=mixer_gain, query_weight=query_weight, key_weight=key_weight, value_weight=value_weight, input_gate=input_gate, forget_gate=forget_gate, head_gain=head_gain, mixer_out_weight=mixer_out_weight, expert_in=expert_in, expert_gain=expert_gain, group_router=group_router, expert_router=expert_router, routes=routes, gate_experts=gate_experts, up_experts=up_experts, down_experts=down_experts)


epsilon = 1e-06
highest = lax.Precision.HIGHEST
floor_log = -1e+30

def rms_rows(matrix, gain):
    widened = matrix.astype(jnp.float32)
    scaled = widened * lax.rsqrt(lax.optimization_barrier(jnp.mean(widened * widened, axis=-1, keepdims=True)) + epsilon)
    return scaled * gain

def block_state(keys, value_rows, input_block, forget_block, scale):
    cumulative = jnp.cumsum(forget_block, axis=-1)
    total_log = cumulative[..., -1]
    log_weight = total_log[..., None] - cumulative + input_block
    peak_log = lax.optimization_barrier(jnp.max(log_weight, axis=-1))
    weights = jnp.exp(log_weight - peak_log[..., None])
    key_float = keys.astype(jnp.float32) * scale
    value_weighted = value_rows.astype(jnp.float32) * weights[..., None]
    memory = jnp.einsum('...sv,...sk->...vk', value_weighted, key_float, precision=highest)
    return (memory, peak_log, total_log)

def merge_state(earlier, later):
    peak_log = jnp.maximum(later[2] + earlier[1], later[1])
    fade_earlier = jnp.exp(later[2] + earlier[1] - peak_log)
    fade_later = jnp.exp(later[1] - peak_log)
    memory = fade_earlier[..., None, None] * earlier[0] + fade_later[..., None, None] * later[0]
    return (memory, peak_log, earlier[2] + later[2])

def block_out(queries, keys, value_rows, input_block, forget_block, state, scale):
    cumulative = jnp.cumsum(forget_block, axis=-1)
    length = cumulative.shape[-1]
    causal = jnp.tril(jnp.ones((length, length), dtype=bool))
    within = jnp.where(causal, cumulative[..., :, None] - cumulative[..., None, :] + input_block[..., None, :], -jnp.inf)
    carried = cumulative + state[1][..., None]
    highest_log = jnp.maximum(lax.optimization_barrier(jnp.max(within, axis=-1)), carried)
    weight_within = jnp.exp(within - highest_log[..., None])
    weight_carried = jnp.exp(carried - highest_log)
    raw_scores = jnp.einsum('...td,...sd->...ts', queries.astype(jnp.float32), keys.astype(jnp.float32)) * scale
    block_scores = raw_scores * weight_within
    rounded = lax.optimization_barrier(block_scores.astype(jnp.bfloat16)).astype(jnp.float32)
    numerator = jnp.einsum('...ts,...sd->...td', rounded, value_rows.astype(jnp.float32))
    query_float = queries.astype(jnp.float32)
    return numerator + weight_carried[..., None] * jnp.einsum('...vk,...tk->...tv', state[0], query_float, precision=highest)

def route_weights(group_logits, expert_logits, routes):
    members = expert_logits.shape[1] // group_logits.shape[1]
    chosen = jnp.take_along_axis(expert_logits, routes, axis=1)
    group_pick = jnp.take_along_axis(group_logits, routes // members, axis=1)
    return jax.nn.sigmoid(group_pick) * jax.nn.sigmoid(chosen - chosen[:, ::-1])

def reference(mixer_in, mixer_gain, query_weight, key_weight, value_weight, input_gate, forget_gate, head_gain, mixer_out_weight, expert_in, expert_gain, group_router, expert_router, routes, gate_experts, up_experts, down_experts):
    normed_a = rms_rows(mixer_in, mixer_gain).astype(jnp.bfloat16)
    queries = jnp.dot(normed_a, query_weight, preferred_element_type=jnp.float32).astype(jnp.bfloat16)
    keys = jnp.dot(normed_a, key_weight, preferred_element_type=jnp.float32).astype(jnp.bfloat16)
    value_rows = jnp.dot(normed_a, value_weight, preferred_element_type=jnp.float32).astype(jnp.bfloat16)
    sequence = normed_a.shape[0]
    head_count = input_gate.shape[0]
    width = queries.shape[1]
    head_size = width // head_count
    block_count = sequence // BLOCK
    scale = head_size ** (-0.5)

    def split_heads(matrix):
        return matrix.reshape(block_count, BLOCK, head_count, head_size).transpose(0, 2, 1, 3)

    def split_gates(gates):
        return gates.reshape(head_count, block_count, BLOCK).transpose(1, 0, 2)
    initial = (jnp.zeros((head_count, head_size, head_size), jnp.float32), jnp.full((head_count,), floor_log, jnp.float32), jnp.zeros((head_count,), jnp.float32))

    def block_step(state, block_data):
        query_block, key_block, value_block, input_block, forget_block = block_data
        output = block_out(query_block, key_block, value_block, input_block, forget_block, state, scale)
        updated = merge_state(state, block_state(key_block, value_block, input_block, forget_block, scale))
        return (updated, output)
    outcome = lax.scan(block_step, initial, (split_heads(queries), split_heads(keys), split_heads(value_rows), split_gates(input_gate), split_gates(jax.nn.log_sigmoid(forget_gate))))
    cells = outcome[1].transpose(0, 2, 1, 3).reshape(sequence, head_count, head_size)
    cell_rows = rms_rows(cells, head_gain.reshape(head_count, head_size)).reshape(sequence, width).astype(jnp.bfloat16)
    group_width = width // N_TP
    mixed = jnp.zeros((sequence, mixer_out_weight.shape[1]), jnp.float32)
    for group in range(N_TP):
        partial_value = jnp.dot(cell_rows[:, group * group_width:(group + 1) * group_width], mixer_out_weight[group * group_width:(group + 1) * group_width], preferred_element_type=jnp.float32).astype(jnp.bfloat16)
        mixed = mixed + lax.optimization_barrier(partial_value).astype(jnp.float32)
    mixer_out = mixed.astype(jnp.bfloat16)
    normed_b = rms_rows(expert_in, expert_gain).astype(jnp.bfloat16)
    group_logits = jnp.dot(normed_b, group_router, preferred_element_type=jnp.float32)
    expert_logits = jnp.dot(normed_b, expert_router, preferred_element_type=jnp.float32)
    combine = route_weights(group_logits, expert_logits, routes)
    token_count = normed_b.shape[0]
    expert_total = expert_logits.shape[1]
    token_device = token_count // N_EP
    capacity = 4 * token_device // expert_total
    flat_routes = routes.reshape(-1)
    pair_total = flat_routes.shape[0]
    matches = (flat_routes.reshape(N_EP, 2 * token_device)[:, :, None] == jnp.arange(expert_total, dtype=jnp.int32)[None, None, :]).astype(jnp.int32)
    sequence_place = (lax.optimization_barrier(jnp.sum(jnp.cumsum(matches, axis=1) * matches, axis=2)) - 1).reshape(-1)
    source = jnp.arange(pair_total, dtype=jnp.int32) // (2 * token_device)
    slot_index = source * capacity + sequence_place
    owner = jnp.full((expert_total, N_EP * capacity), pair_total, jnp.int32).at[flat_routes, slot_index].set(jnp.arange(pair_total, dtype=jnp.int32))
    padded = jnp.concatenate([normed_b, jnp.zeros((1, normed_b.shape[1]), jnp.bfloat16)], axis=0)
    weights_flat = jnp.concatenate([combine.reshape(-1), jnp.zeros((1,), jnp.float32)])
    hidden_group = gate_experts.shape[2] // N_TP

    def expert_step(total_out, expert_data):
        owners, gate_weight, up_weight, down_weight = expert_data
        rows_in = padded[owners // 2]
        gate_act = jnp.dot(rows_in, gate_weight, preferred_element_type=jnp.float32)
        up_act = jnp.dot(rows_in, up_weight, preferred_element_type=jnp.float32)
        hidden = (jax.nn.silu(gate_act) * up_act).astype(jnp.bfloat16)
        summed = jnp.zeros((rows_in.shape[0], down_weight.shape[1]), jnp.float32)
        for group in range(N_TP):
            partial_value = jnp.dot(hidden[:, group * hidden_group:(group + 1) * hidden_group], down_weight[group * hidden_group:(group + 1) * hidden_group], preferred_element_type=jnp.float32).astype(jnp.bfloat16)
            summed = summed + lax.optimization_barrier(partial_value).astype(jnp.float32)
        result = lax.optimization_barrier(summed.astype(jnp.bfloat16)).astype(jnp.float32)
        total_out = total_out.at[owners // 2].add(weights_flat[owners][:, None] * result)
        return (total_out, None)
    finished = lax.scan(expert_step, jnp.zeros((token_count + 1, normed_b.shape[1]), jnp.float32), (owner, gate_experts, up_experts, down_experts))
    expert_out = finished[0][:token_count].astype(jnp.bfloat16)
    return (mixer_out, expert_out)
```

```python
import jax
import jax.numpy as jnp
from jax import lax
from jax.experimental import pallas as pl
from jax.experimental.pallas import tpu as pltpu
from jax.sharding import Mesh
from jax.sharding import PartitionSpec as P

BLOCK = 128
EP = ("z", "y", "c")
EP_TP = ("z", "y", "c", "tp")
ZY = ("z", "y")
LEFT = [(i, (i - 1) % 4) for i in range(4)]
RIGHT = [(i, (i + 1) % 4) for i in range(4)]
SWAP = [(0, 1), (1, 0)]
f32 = jnp.float32
bf16 = jnp.bfloat16

epsilon = 1e-06
highest = lax.Precision.HIGHEST
floor_log = -1e30


def rms_rows(matrix, gain):
    widened = matrix.astype(f32)
    scaled = widened * lax.rsqrt(jnp.mean(widened * widened, axis=-1, keepdims=True) + epsilon)
    return scaled * gain


def block_state(keys, value_rows, input_block, forget_block, scale):
    cumulative = jnp.cumsum(forget_block, axis=-1)
    total_log = cumulative[..., -1]
    log_weight = total_log[..., None] - cumulative + input_block
    peak_log = jnp.max(log_weight, axis=-1)
    weights = jnp.exp(log_weight - peak_log[..., None])
    key_float = keys.astype(f32) * scale
    value_weighted = value_rows.astype(f32) * weights[..., None]
    memory = jnp.einsum("...sv,...sk->...vk", value_weighted, key_float, precision=highest)
    return (memory, peak_log, total_log)


def merge_state(earlier, later):
    peak_log = jnp.maximum(later[2] + earlier[1], later[1])
    fade_earlier = jnp.exp(later[2] + earlier[1] - peak_log)
    fade_later = jnp.exp(later[1] - peak_log)
    memory = fade_earlier[..., None, None] * earlier[0] + fade_later[..., None, None] * later[0]
    return (memory, peak_log, earlier[2] + later[2])


def block_out(queries, keys, value_rows, input_block, forget_block, state, scale):
    cumulative = jnp.cumsum(forget_block, axis=-1)
    length = cumulative.shape[-1]
    causal = jnp.tril(jnp.ones((length, length), dtype=bool))
    within = jnp.where(
        causal,
        cumulative[..., :, None] - cumulative[..., None, :] + input_block[..., None, :],
        -jnp.inf,
    )
    carried = cumulative + state[1][..., None]
    highest_log = jnp.maximum(jnp.max(within, axis=-1), carried)
    weight_within = jnp.exp(within - highest_log[..., None])
    weight_carried = jnp.exp(carried - highest_log)
    raw_scores = jnp.einsum("...td,...sd->...ts", queries, keys, preferred_element_type=f32) * scale
    block_scores = raw_scores * weight_within
    numerator = jnp.einsum(
        "...ts,...sd->...td", block_scores.astype(bf16), value_rows, preferred_element_type=f32
    )
    query_float = queries.astype(f32)
    return numerator + weight_carried[..., None] * jnp.einsum(
        "...vk,...tk->...tv", state[0], query_float, precision=highest
    )


def take_block(states, block_index):
    return tuple((member[block_index] for member in states))


def packed(summary):
    row = lax.broadcasted_iota(jnp.int32, (8, 128), 0)
    tail = jnp.where(row == 0, summary[1], jnp.where(row == 1, summary[2], 0.0))
    return jnp.concatenate([summary[0], tail], axis=0)


def unpacked(lines, valid=None):
    memory, peak, total = lines[:128], lines[128, 0], lines[129, 0]
    if valid is None:
        return (memory, peak, total)
    return (
        jnp.where(valid, memory, 0.0),
        jnp.where(valid, peak, floor_log),
        jnp.where(valid, total, 0.0),
    )


def sent(summary, axis, pairs):
    return lax.ppermute(packed(summary), axis, pairs)


def state_before(summary):
    z, y, c = (lax.axis_index(a) for a in EP)
    first = c == 0

    def head(k):
        return tuple(lax.dynamic_index_in_dim(m, k, 0, keepdims=False) for m in summary)

    def pick(flag, a, b):
        return jax.tree.map(lambda p, q: jnp.where(flag, p, q), a, b)

    own = head(c)
    other = unpacked(sent(head(1 - c), "c", SWAP))
    earlier_core = pick(first, own, other)
    chip = merge_state(earlier_core, pick(first, other, own))
    rings = {k: sent(chip, "y", [(i, (i + k) % 4) for i in range(4)]) for k in (1, 2, 3)}
    before_y = unpacked(rings[3], y >= 3)
    for k in (2, 1):
        before_y = merge_state(before_y, unpacked(rings[k], y >= k))
    slab = merge_state(before_y, chip)
    for k in (3, 2, 1):
        slab = merge_state(slab, unpacked(rings[k], y + 4 - k <= 3))
    lines = {k: sent(slab, "z", [(i, i + k) for i in range(8 - k)]) for k in (1, 2, 3)}
    near = unpacked(lines[3], z >= 3)
    for k in (2, 1):
        near = merge_state(near, unpacked(lines[k], z >= k))
    far = unpacked(
        sent(merge_state(near, slab), "z", [(i, i + 4) for i in range(4)]), z >= 4
    )
    start = merge_state(merge_state(far, near), before_y)
    second = merge_state(start, earlier_core)
    mine = pick(first, start, second)
    theirs = unpacked(sent(pick(first, second, start), "c", SWAP))
    return jax.tree.map(
        lambda a, b: jnp.where(first, jnp.stack([a, b]), jnp.stack([b, a])), mine, theirs
    )


def around_ring(x):
    half = x.shape[0] // 2
    right = lax.ppermute(x, "tp", LEFT)
    left = lax.ppermute(x, "tp", RIGHT)
    upper = lax.ppermute(right[:half], "tp", LEFT)
    lower = lax.ppermute(left[half:], "tp", RIGHT)
    return (x, right, upper, lower, left)


def exchanged(x, dim, size):
    rank = lax.axis_index("tp")
    pieces = []
    for k in range(4):
        piece = lax.dynamic_slice_in_dim(x, ((rank - k) % 4) * size, size, dim)
        pieces.append(piece if k == 0 else lax.ppermute(piece, "tp", [(i, (i - k) % 4) for i in range(4)]))
    return pieces


def dispatch_kernel(place, rows, gain, group_router, expert_router, routes, own, other, notes, normed):
    rank, core = place[0], place[1]
    x = rows[...].astype(f32)
    scaled = x * lax.rsqrt(jnp.mean(x * x, axis=-1, keepdims=True) + epsilon)
    normed[...] = (scaled * gain[...]).astype(bf16)
    group_logits = jnp.dot(normed[...], group_router[...], preferred_element_type=f32)
    expert_logits = jnp.dot(normed[...], expert_router[...], preferred_element_type=f32)
    tokens, experts = expert_logits.shape
    groups = group_logits.shape[1]
    expert_ids = lax.broadcasted_iota(jnp.int32, (tokens, experts), 1)
    group_ids = lax.broadcasted_iota(jnp.int32, (tokens, groups), 1)
    table = routes[...]
    named = [table[:, k : k + 1] for k in range(2)]
    hot = [(expert_ids == e).astype(f32) for e in named]
    below = (
        lax.broadcasted_iota(jnp.int32, (tokens, tokens), 1)
        < lax.broadcasted_iota(jnp.int32, (tokens, tokens), 0)
    ).astype(bf16)
    counts = [jnp.dot(below, h.astype(bf16), preferred_element_type=f32) for h in hot]
    counts[1] = counts[1] + jnp.sum(hot[0], axis=0, keepdims=True)
    slots = []
    for k in range(2):
        at = jnp.sum(hot[k] * counts[k], axis=1, keepdims=True).astype(jnp.int32)
        slots.append((((named[k] & 1) ^ core) * (experts // 2) + (named[k] >> 1)) * 16 + at)
    chosen = [jnp.sum(h * expert_logits, axis=1, keepdims=True) for h in hot]
    grouped = [
        jnp.sum(jnp.where(group_ids == e // (experts // groups), group_logits, 0.0), axis=1, keepdims=True)
        for e in named
    ]
    combine = [
        jax.nn.sigmoid(grouped[k]) * jax.nn.sigmoid(chosen[k] - chosen[1 - k]) for k in range(2)
    ]
    lane = lax.broadcasted_iota(jnp.int32, (tokens, 128), 1)
    wide = jnp.where(lane == 0, slots[0].astype(f32), slots[1].astype(f32))
    notes[...] = jnp.where(lane < 2, wide, jnp.where(lane == 2, combine[0], combine[1]))
    across = wide.T
    first, second = (across[k : k + 1].astype(jnp.int32) for k in range(2))
    share = rows.shape[1] // 4
    features = normed[:, pl.ds(pl.multiple_of(rank * share, share), share)]
    half = own.shape[0]
    slot_ids = lax.broadcasted_iota(jnp.int32, (half, tokens), 0)
    for j, target in enumerate((own, other)):
        pick = ((slot_ids + j * half == first) | (slot_ids + j * half == second)).astype(bf16)
        target[...] = jnp.dot(pick, features, preferred_element_type=f32).astype(bf16)


def hidden_kernel(place, own, right, upper, lower, left, gate, up, out):
    share = own.shape[1]
    half = upper.shape[0]

    def term(k, rows):
        at = pl.ds(pl.multiple_of(((place[0] + k) % 4) * share, share), share)
        return (
            jnp.dot(rows, gate[at, :], preferred_element_type=f32),
            jnp.dot(rows, up[at, :], preferred_element_type=f32),
        )

    for part, across in ((0, upper), (1, lower)):
        rows = pl.ds(part * half, half)
        terms = [
            term(0, own[rows, :]),
            term(1, right[rows, :]),
            term(2, across[...]),
            term(3, left[rows, :]),
        ]
        gate_act = terms[0][0] + terms[1][0] + terms[2][0] + terms[3][0]
        up_act = terms[0][1] + terms[1][1] + terms[2][1] + terms[3][1]
        out[rows, :] = (jax.nn.silu(gate_act) * up_act).astype(bf16)


def down_kernel(own, right, upper, lower, left, w0, w1, w2, w3, out):
    half = upper.shape[0]
    for part, across in ((0, upper), (1, lower)):
        rows = pl.ds(part * half, half)
        total = jnp.dot(own[rows, :], w0[...], preferred_element_type=f32)
        total = total + jnp.dot(right[rows, :], w1[...], preferred_element_type=f32)
        total = total + jnp.dot(across[...], w2[...], preferred_element_type=f32)
        total = total + jnp.dot(left[rows, :], w3[...], preferred_element_type=f32)
        out[rows, :] = total.astype(bf16)


def combine_kernel(notes, own, other, out):
    half = own.shape[0]
    tokens = out.shape[0]
    slots = [notes[:, k : k + 1].astype(jnp.int32) for k in range(2)]
    combine = [notes[:, k : k + 1] for k in (2, 3)]
    lanes = lax.broadcasted_iota(jnp.int32, (tokens, half), 1)
    total = jnp.zeros(out.shape, f32)
    for j, rows in enumerate((own, other)):
        weight = jnp.where(lanes + j * half == slots[0], combine[0], 0.0) + jnp.where(
            lanes + j * half == slots[1], combine[1], 0.0
        )
        high = weight.astype(bf16)
        low = (weight - high.astype(f32)).astype(bf16)
        total = total + jnp.dot(high, rows[...], preferred_element_type=f32)
        total = total + jnp.dot(low, rows[...], preferred_element_type=f32)
    out[...] = total.astype(bf16)


def whole(count):
    return [pl.BlockSpec(memory_space=pltpu.VMEM)] * count


def scalars():
    return [pl.BlockSpec(memory_space=pltpu.SMEM)]


PARAMS = pltpu.CompilerParams(vmem_limit_bytes=48 * 1024 * 1024)


def shards(
    mixer_in,
    mixer_gain,
    query_weight,
    key_weight,
    value_weight,
    input_gate,
    forget_gate,
    head_gain,
    mixer_out_weight,
    expert_in,
    expert_gain,
    group_router,
    expert_router,
    routes,
    gate_experts,
    up_experts,
    down_experts,
):
    rank, core = lax.axis_index("tp"), lax.axis_index("c")
    place = jnp.stack([rank, core]).astype(jnp.int32)
    tokens, width = expert_in.shape
    share = width // 4
    slots = 32 * 16
    send_own, send_other, notes = pl.pallas_call(
        dispatch_kernel,
        out_shape=(
            jax.ShapeDtypeStruct((slots, share), bf16),
            jax.ShapeDtypeStruct((slots, share), bf16),
            jax.ShapeDtypeStruct((tokens, 128), f32),
        ),
        in_specs=scalars() + whole(5),
        out_specs=tuple(whole(3)),
        scratch_shapes=[pltpu.VMEM((tokens, width), bf16)],
        compiler_params=PARAMS,
        name="dispatch",
    )(place, expert_in, expert_gain.reshape(1, -1), group_router, expert_router, routes)

    swapped = lax.ppermute(send_other, "c", SWAP)
    arrived = [lax.all_to_all(s, ZY, 0, 0, tiled=True) for s in (send_own, swapped)]

    down_parts = exchanged(down_experts[0], 1, share)
    half_weight = lax.dynamic_slice_in_dim(mixer_out_weight, core * 128, 128, 0)
    ring_weight = around_ring(half_weight)
    other_weight = [lax.ppermute(piece, "c", SWAP) for piece in ring_weight]

    gate, up = gate_experts[0], up_experts[0]
    results = []
    for rows in arrived:
        hidden = pl.pallas_call(
            hidden_kernel,
            out_shape=jax.ShapeDtypeStruct((slots, gate.shape[1]), bf16),
            in_specs=scalars() + whole(7),
            out_specs=whole(1)[0],
            compiler_params=PARAMS,
            name="hidden",
        )(place, *around_ring(rows), gate, up)
        results.append(
            pl.pallas_call(
                down_kernel,
                out_shape=jax.ShapeDtypeStruct((slots, share), bf16),
                in_specs=whole(9),
                out_specs=whole(1)[0],
                compiler_params=PARAMS,
                name="down",
            )(*around_ring(hidden), *down_parts)
        )
    back_own, back_other = (lax.all_to_all(r, ZY, 0, 0, tiled=True) for r in results)
    back_other = lax.ppermute(back_other, "c", SWAP)
    expert_out = pl.pallas_call(
        combine_kernel,
        out_shape=jax.ShapeDtypeStruct((tokens, share), bf16),
        in_specs=whole(3),
        out_specs=whole(1)[0],
        compiler_params=PARAMS,
        name="combine",
    )(notes, back_own, back_other)

    normed_a = rms_rows(mixer_in, mixer_gain).astype(bf16)
    queries = jnp.dot(normed_a, query_weight, preferred_element_type=f32).astype(bf16)
    keys = jnp.dot(normed_a, key_weight, preferred_element_type=f32).astype(bf16)
    value_rows = jnp.dot(normed_a, value_weight, preferred_element_type=f32).astype(bf16)
    row_count = normed_a.shape[0]
    head_local = input_gate.shape[0]
    width_local = queries.shape[1]
    head_size = width_local // head_local
    block_count = row_count // BLOCK
    scale = head_size ** (-0.5)

    def split_heads(matrix):
        return matrix.reshape(block_count, BLOCK, head_local, head_size).transpose(0, 2, 1, 3)

    def split_gates(gates):
        return gates.reshape(head_local, block_count, BLOCK).transpose(1, 0, 2)

    query_blocks = split_heads(queries)
    key_blocks = split_heads(keys)
    value_blocks = split_heads(value_rows)
    input_blocks = split_gates(input_gate)
    forget_blocks = split_gates(jax.nn.log_sigmoid(forget_gate))
    summaries = block_state(key_blocks, value_blocks, input_blocks, forget_blocks, scale)
    summary = take_block(summaries, 0)
    for block_index in range(1, block_count):
        summary = merge_state(summary, take_block(summaries, block_index))
    current = state_before(summary)
    start_list = [current]
    for block_index in range(block_count - 1):
        current = merge_state(current, take_block(summaries, block_index))
        start_list.append(current)
    starts = tuple((jnp.stack([entry[member] for entry in start_list]) for member in range(3)))
    cells = block_out(
        query_blocks, key_blocks, value_blocks, input_blocks, forget_blocks, starts, scale
    )
    cells = cells.transpose(0, 2, 1, 3).reshape(row_count, head_local, head_size)
    gain_local = lax.dynamic_slice_in_dim(head_gain, rank * width_local, width_local).reshape(
        head_local, head_size
    )
    cell_rows = rms_rows(cells, gain_local).reshape(row_count, width_local).astype(bf16)

    cell_parts = exchanged(cell_rows, 0, row_count // 4)

    def both_halves(mine, theirs):
        pair = jnp.stack([mine, theirs])
        return lax.dynamic_index_in_dim(pair, core, 0, False), lax.dynamic_index_in_dim(
            pair, 1 - core, 0, False
        )

    def in_order(pieces):
        return (pieces[0], pieces[1], jnp.concatenate([pieces[2], pieces[3]], axis=0), pieces[4])

    mixed = jnp.zeros((row_count // 4, width), f32)
    for cell, mine, theirs in zip(cell_parts, in_order(ring_weight), in_order(other_weight)):
        low, high = both_halves(mine, theirs)
        weight = jnp.concatenate([low, high], axis=0)
        mixed = mixed + jnp.dot(cell, weight, preferred_element_type=f32).astype(bf16).astype(f32)
    return (mixed.astype(bf16), expert_out)


def solution(mesh):
    split = Mesh(mesh.devices.reshape(8, 4, 2, mesh.shape["tp"]), EP_TP)
    placed = (
        P(EP, None),
        P(),
        P(None, "tp"),
        P(None, "tp"),
        P(None, "tp"),
        P("tp", EP),
        P("tp", EP),
        P(),
        P("tp", None),
        P(EP, None),
        P(),
        P(),
        P(),
        P(EP, None),
        P(EP, None, "tp"),
        P(EP, None, "tp"),
        P(EP, "tp", None),
    )
    return jax.shard_map(
        shards,
        mesh=split,
        in_specs=placed,
        out_specs=(P(EP_TP, None), P(EP, "tp")),
        check_vma=False,
    )
```

```python
import jax
import jax.numpy as jnp
from jax import lax
from jax.experimental import pallas as pl
from jax.experimental.pallas import tpu as pltpu
from jax.sharding import Mesh
from jax.sharding import PartitionSpec as P

EP = ("z", "y", "c")
EP_TP = ("z", "y", "c", "tp")
ZY = ("z", "y")
YC = ("y", "c")
NEAR = [(i, i ^ 1) for i in range(4)]
FAR = [(i, 3 - i) for i in range(4)]
ACROSS = [(i, i ^ 2) for i in range(4)]
SWAP = [(0, 1), (1, 0)]
CROSS = [(c * 4 + t, (c if t < 2 else 1 - c) * 4 + t) for c in range(2) for t in range(4)]
LINES = 136
f32 = jnp.float32
bf16 = jnp.bfloat16

epsilon = 1e-06
highest = lax.Precision.HIGHEST
floor_log = -1e30


def normalized(matrix):
    return matrix * lax.rsqrt(jnp.mean(matrix * matrix, axis=-1, keepdims=True) + epsilon)


def thirds(x):
    high = x.astype(bf16)
    rest = x - high.astype(f32)
    middle = rest.astype(bf16)
    return high, middle, (rest - middle.astype(f32)).astype(bf16)


def merged(earlier, later):
    moved = later[2] + earlier[1]
    peak = jnp.maximum(moved, later[1])
    memory = jnp.exp(moved - peak) * earlier[0] + jnp.exp(later[1] - peak) * later[0]
    return (memory, peak, earlier[2] + later[2])


def summary_at(ref, base):
    return (ref[base : base + 128, :], ref[base + 128 : base + 129, :], ref[base + 129 : base + 130, :])


def put_summary(ref, base, summary):
    row = lax.broadcasted_iota(jnp.int32, (8, 128), 0)
    ref[base : base + 128, :] = summary[0]
    ref[base + 128 : base + 136, :] = jnp.where(
        row == 0, summary[1], jnp.where(row == 1, summary[2], 0.0)
    )


def no_summary():
    return (jnp.zeros((128, 128), f32), jnp.full((1, 128), floor_log, f32), jnp.zeros((1, 128), f32))


def chosen_summary(flag, a, b):
    return tuple(jnp.where(flag, p, q) for p, q in zip(a, b))


def gate_sums(log_forget, input_gate):
    s = lax.broadcasted_iota(jnp.int32, (128, 128), 0)
    t = lax.broadcasted_iota(jnp.int32, (128, 128), 1)
    upto = (s <= t).astype(f32)
    sums = jnp.dot(log_forget[...], upto, preferred_element_type=f32, precision=highest)
    total = jnp.sum(log_forget[...], axis=1, keepdims=True)
    log_weight = total - sums + input_gate[...]
    peak = jnp.max(log_weight, axis=1, keepdims=True)
    return sums, total, log_weight, peak


def as_columns(rows):
    return jnp.concatenate([rows, jnp.zeros((120, 128), f32)], axis=0).T


def mixer_head_kernel(rows, gain, wq, wk, wv, log_forget, input_gate, q, k, v, memories, spread, normed):
    normed[...] = (normalized(rows[...].astype(f32)) * gain[...]).astype(bf16)
    for weight, target in ((wq, q), (wk, k), (wv, v)):
        target[...] = jnp.dot(normed[...], weight[...], preferred_element_type=f32).astype(bf16)
    _, total, log_weight, peak = gate_sums(log_forget, input_gate)
    columns = as_columns(jnp.exp(log_weight - peak))
    for h in range(2):
        whole_summary = None
        for b in range(4):
            n = h * 4 + b
            at = (slice(b * 128, b * 128 + 128), slice(h * 128, h * 128 + 128))
            keys = k[at].astype(f32).T.astype(bf16)
            weighted = v[at].astype(f32) * columns[:, n : n + 1]
            parts = [jnp.dot(keys, p, preferred_element_type=f32) for p in thirds(weighted)]
            memory = (parts[2] + parts[1] + parts[0]) * 128**-0.5
            memories[n * 128 : n * 128 + 128, :] = memory
            ones = jnp.ones((1, 128), f32)
            summary = (memory, peak[n : n + 1, :] * ones, total[n : n + 1, :] * ones)
            whole_summary = summary if b == 0 else merged(whole_summary, summary)
        for y in range(4):
            put_summary(spread, (2 * y + h) * LINES, whole_summary)


def fold_slab_kernel(place, members, spread, before):
    running = no_summary()
    captured = [no_summary(), no_summary()]
    for n in range(8):
        captured[n % 2] = chosen_summary(place[3] == n // 2, running, captured[n % 2])
        running = merged(running, summary_at(members, n * LINES))
    for n in range(8):
        put_summary(spread, n * LINES, running)
    for n in range(2):
        put_summary(before, n * LINES, captured[n])


def fold_all_kernel(place, slabs, before, mine, theirs):
    running = no_summary()
    start = no_summary()
    for n in range(8):
        start = chosen_summary(place[2] == n, running, start)
        if n < 7:
            running = merged(running, summary_at(slabs, n * LINES))
    pair = [merged(start, summary_at(before, n * LINES)) for n in range(2)]
    put_summary(mine, 0, chosen_summary(place[1] == 0, pair[0], pair[1]))
    put_summary(theirs, 0, chosen_summary(place[1] == 0, pair[1], pair[0]))


def mixer_tail_kernel(
    place, q, k, v, log_forget, input_gate, memories, mine, theirs, gain, weight,
    own, near, far, across_near, across_far, cells
):
    sums, total, _, peak = gate_sums(log_forget, input_gate)
    columns = as_columns(sums)
    later = lax.broadcasted_iota(jnp.int32, (128, 128), 1) > lax.broadcasted_iota(
        jnp.int32, (128, 128), 0
    )
    ones = jnp.ones((1, 128), f32)
    for h in range(2):
        state = chosen_summary(place[1] == h, summary_at(mine, 0), summary_at(theirs, 0))
        head_gain = gain[:, pl.ds(pl.multiple_of(place[0] * 256 + h * 128, 128), 128)]
        for b in range(4):
            n = h * 4 + b
            at = (slice(b * 128, b * 128 + 128), slice(h * 128, h * 128 + 128))
            column = columns[:, n : n + 1]
            within = column - sums[n : n + 1, :] + input_gate[n : n + 1, :]
            within = jnp.where(later, floor_log, within)
            carried = column + state[1][:, 0:1]
            top = jnp.maximum(jnp.max(within, axis=1, keepdims=True), carried)
            raw = lax.dot_general(
                q[at], k[at], (((1,), (1,)), ((), ())), preferred_element_type=f32
            )
            scores = raw * 128**-0.5 * jnp.exp(within - top)
            scores = jnp.where(later, 0.0, scores).astype(bf16)
            inside = jnp.dot(scores, v[at], preferred_element_type=f32)
            parts = [jnp.dot(q[at], p, preferred_element_type=f32) for p in thirds(state[0])]
            outside = parts[2] + parts[1] + parts[0]
            cell = inside + jnp.exp(carried - top) * outside
            cells[at] = (normalized(cell) * head_gain).astype(bf16)
            if b < 3:
                block = (memories[n * 128 : n * 128 + 128, :], peak[n : n + 1, :] * ones, total[n : n + 1, :] * ones)
                state = merged(state, block)
    count = own.shape[0]
    rank = place[0]
    for target, device, start in (
        (own, rank, 0),
        (near, rank ^ 1, 0),
        (far, 3 - rank, 0),
        (across_near, rank ^ 2, 0),
        (across_far, rank ^ 2, count // 2),
    ):
        at = pl.ds(pl.multiple_of(device * count + start, count // 2), target.shape[0])
        target[...] = jnp.dot(cells[at, :], weight[...], preferred_element_type=f32).astype(bf16)


def relay_kernel(near, far, from_near, from_far, to_near, to_far):
    half = from_near.shape[0]
    to_far[:half, :] = (far[:half, :].astype(f32) + from_near[...].astype(f32)).astype(bf16)
    to_far[half:, :] = far[half:, :]
    to_near[:half, :] = near[:half, :]
    to_near[half:, :] = (near[half:, :].astype(f32) + from_far[...].astype(f32)).astype(bf16)


def sum_kernel(own, near, far, out):
    total = own[...].astype(f32) + near[...].astype(f32) + far[...].astype(f32)
    out[...] = total.astype(bf16)


def cut_kernel(place, weights, own, near, far, across):
    rank = place[0]
    share = weights.shape[1] // 4
    for target, device in ((own, rank), (near, rank ^ 1), (far, 3 - rank), (across, rank ^ 2)):
        for j, quarter in enumerate((device, 3 - device)):
            target[:, j * share : (j + 1) * share] = weights[
                :, pl.ds(pl.multiple_of(quarter * share, share), share)
            ]


def dispatch_kernel(place, rows, gain, group_router, expert_router, routes, send, notes, normed):
    rank, core = place[0], place[1]
    normed[...] = (normalized(rows[...].astype(f32)) * gain[...]).astype(bf16)
    group_logits = jnp.dot(normed[...], group_router[...], preferred_element_type=f32)
    expert_logits = jnp.dot(normed[...], expert_router[...], preferred_element_type=f32)
    tokens, experts = expert_logits.shape
    groups = group_logits.shape[1]
    expert_ids = lax.broadcasted_iota(jnp.int32, (tokens, experts), 1)
    group_ids = lax.broadcasted_iota(jnp.int32, (tokens, groups), 1)
    table = routes[...]
    named = [table[:, k : k + 1] for k in range(2)]
    hot = [(expert_ids == e).astype(f32) for e in named]
    below = (
        lax.broadcasted_iota(jnp.int32, (tokens, tokens), 1)
        < lax.broadcasted_iota(jnp.int32, (tokens, tokens), 0)
    ).astype(bf16)
    counts = [jnp.dot(below, h.astype(bf16), preferred_element_type=f32) for h in hot]
    counts[1] = counts[1] + jnp.sum(hot[0], axis=0, keepdims=True)
    slots = []
    for k in range(2):
        at = jnp.sum(hot[k] * counts[k], axis=1, keepdims=True).astype(jnp.int32)
        here = ((named[k] & 1) ^ core) == rank // 2
        slots.append(jnp.where(here, (named[k] >> 1) * 16 + at, -1))
    chosen = [jnp.sum(h * expert_logits, axis=1, keepdims=True) for h in hot]
    grouped = [
        jnp.sum(jnp.where(group_ids == e // (experts // groups), group_logits, 0.0), axis=1, keepdims=True)
        for e in named
    ]
    combine = [
        jax.nn.sigmoid(grouped[k]) * jax.nn.sigmoid(chosen[k] - chosen[1 - k]) for k in range(2)
    ]
    lane = lax.broadcasted_iota(jnp.int32, (tokens, 128), 1)
    wide = jnp.where(lane == 0, slots[0].astype(f32), slots[1].astype(f32))
    notes[...] = jnp.where(lane < 2, wide, jnp.where(lane == 2, combine[0], combine[1]))
    across = wide.T
    first, second = (across[k : k + 1].astype(jnp.int32) for k in range(2))
    share = rows.shape[1] // 4
    slot_ids = lax.broadcasted_iota(jnp.int32, (send.shape[0], tokens), 0)
    pick = ((slot_ids == first) | (slot_ids == second)).astype(bf16)
    for j, quarter in enumerate((rank, 3 - rank)):
        features = normed[:, pl.ds(pl.multiple_of(quarter * share, share), share)]
        send[:, j * share : (j + 1) * share] = jnp.dot(
            pick, features, preferred_element_type=f32
        ).astype(bf16)


def hidden_kernel(place, own, other, gate, up, far_gate, far_up, out):
    rank = place[0]
    share = own.shape[1] // 2
    units = gate.shape[1]
    blocks = [
        (own, 0, rank),
        (own, 1, 3 - rank),
        (other, 0, rank ^ 1),
        (other, 1, 3 - (rank ^ 1)),
    ]
    for part, (g, u) in enumerate(((gate, up), (far_gate, far_up))):
        gate_act = up_act = None
        for rows, half, quarter in blocks:
            features = rows[:, half * share : (half + 1) * share]
            at = pl.ds(pl.multiple_of(quarter * share, share), share)
            a = jnp.dot(features, g[at, :], preferred_element_type=f32)
            b = jnp.dot(features, u[at, :], preferred_element_type=f32)
            gate_act = a if gate_act is None else gate_act + a
            up_act = b if up_act is None else up_act + b
        out[:, part * units : (part + 1) * units] = (jax.nn.silu(gate_act) * up_act).astype(bf16)


def down_kernel(own, other, w_own, w_far, w_near, w_across, out):
    units = own.shape[1] // 2
    total = jnp.dot(own[:, :units], w_own[...], preferred_element_type=f32)
    total = total + jnp.dot(own[:, units:], w_far[...], preferred_element_type=f32)
    total = total + jnp.dot(other[:, :units], w_near[...], preferred_element_type=f32)
    total = total + jnp.dot(other[:, units:], w_across[...], preferred_element_type=f32)
    out[...] = total.astype(bf16)


def combine_kernel(notes, rows, keep, send):
    tokens, share = keep.shape
    slots = [notes[:, k : k + 1].astype(jnp.int32) for k in range(2)]
    lanes = lax.broadcasted_iota(jnp.int32, (tokens, rows.shape[0]), 1)
    weight = jnp.where(lanes == slots[0], notes[:, 2:3], 0.0) + jnp.where(
        lanes == slots[1], notes[:, 3:4], 0.0
    )
    high = weight.astype(bf16)
    low = (weight - high.astype(f32)).astype(bf16)
    total = jnp.dot(high, rows[...], preferred_element_type=f32)
    total = total + jnp.dot(low, rows[...], preferred_element_type=f32)
    keep[...] = total[:, :share]
    send[...] = total[:, share:].astype(bf16)


def last_kernel(keep, received, out):
    out[...] = (keep[...] + received[...].astype(f32)).astype(bf16)


def run(kernel, shapes, args, place=None, scratch=()):
    specs = [pl.BlockSpec(memory_space=pltpu.VMEM)] * len(args)
    if place is not None:
        specs = [pl.BlockSpec(memory_space=pltpu.SMEM)] + specs
        args = (place, *args)
    outs = tuple(jax.ShapeDtypeStruct(s, d) for s, d in shapes)
    result = pl.pallas_call(
        kernel,
        out_shape=outs,
        in_specs=specs,
        out_specs=tuple([pl.BlockSpec(memory_space=pltpu.VMEM)] * len(outs)),
        scratch_shapes=[pltpu.VMEM(s, d) for s, d in scratch],
        compiler_params=pltpu.CompilerParams(vmem_limit_bytes=48 * 1024 * 1024),
    )(*args)
    return result if len(outs) > 1 else result[0]


def traded(x, axis):
    return lax.all_to_all(x, axis, 0, 0, tiled=True)


def shards(
    mixer_in,
    mixer_gain,
    query_weight,
    key_weight,
    value_weight,
    input_gate,
    forget_gate,
    head_gain,
    mixer_out_weight,
    expert_in,
    expert_gain,
    group_router,
    expert_router,
    routes,
    gate_experts,
    up_experts,
    down_experts,
):
    place = jnp.stack([lax.axis_index(a) for a in ("tp", "c", "z", "y")]).astype(jnp.int32)
    tokens, width = expert_in.shape
    share = width // 4
    slots = 32 * 16
    gate, up, down = gate_experts[0], up_experts[0], down_experts[0]
    units = gate.shape[1]
    send, notes = run(
        dispatch_kernel,
        (((slots, 2 * share), bf16), ((tokens, 128), f32)),
        (expert_in, expert_gain.reshape(1, -1), group_router, expert_router, routes),
        place,
        [((tokens, width), bf16)],
    )
    send = lax.ppermute(send, ("c", "tp"), CROSS)
    arrived = traded(send, ZY)

    far_gate = lax.ppermute(gate, "tp", FAR)
    far_up = lax.ppermute(up, "tp", FAR)
    w_own, w_near, w_far, w_across = run(
        cut_kernel, (((units, 2 * share), bf16),) * 4, (down,), place
    )
    w_near = lax.ppermute(w_near, "tp", NEAR)
    w_far = lax.ppermute(w_far, "tp", FAR)
    w_across = lax.ppermute(w_across, "tp", ACROSS)

    row_count = mixer_in.shape[0]
    local = query_weight.shape[1]
    log_forget = jax.nn.log_sigmoid(forget_gate).reshape(8, 128)
    inputs = input_gate.reshape(8, 128)
    q, k, v, memories, spread = run(
        mixer_head_kernel,
        (((row_count, local), bf16),) * 3 + (((8 * 128, 128), f32), ((8 * LINES, 128), f32)),
        (mixer_in, mixer_gain.reshape(1, -1), query_weight, key_weight, value_weight, log_forget, inputs),
        None,
        [((row_count, width), bf16)],
    )
    members = traded(spread, YC)
    spread, before = run(
        fold_slab_kernel, (((8 * LINES, 128), f32), ((2 * LINES, 128), f32)), (members,), place
    )
    slabs = traded(spread, "z")
    mine, theirs = run(fold_all_kernel, (((LINES, 128), f32),) * 2, (slabs, before), place)
    theirs = lax.ppermute(theirs, "c", SWAP)
    count = row_count // 4
    own, near, far, across_near, across_far = run(
        mixer_tail_kernel,
        (((count, width), bf16),) * 3 + (((count // 2, width), bf16),) * 2,
        (q, k, v, log_forget, inputs, memories, mine, theirs, head_gain.reshape(1, -1), mixer_out_weight),
        place,
        [((row_count, local), bf16)],
    )
    from_near = lax.ppermute(across_near, "tp", NEAR)
    from_far = lax.ppermute(across_far, "tp", FAR)
    to_near, to_far = run(
        relay_kernel, (((count, width), bf16),) * 2, (near, far, from_near, from_far)
    )
    near = lax.ppermute(to_near, "tp", NEAR)
    far = lax.ppermute(to_far, "tp", FAR)
    mixer_out = run(sum_kernel, (((count, width), bf16),), (own, near, far))

    other_rows = lax.ppermute(arrived, "tp", NEAR)
    hidden = run(
        hidden_kernel,
        (((slots, 2 * units), bf16),),
        (arrived, other_rows, gate, up, far_gate, far_up),
        place,
    )
    other_hidden = lax.ppermute(hidden, "tp", NEAR)
    result = run(
        down_kernel,
        (((slots, 2 * share), bf16),),
        (hidden, other_hidden, w_own, w_far, w_near, w_across),
    )
    back = traded(result, ZY)
    back = lax.ppermute(back, ("c", "tp"), CROSS)
    keep, give = run(
        combine_kernel, (((tokens, share), f32), ((tokens, share), bf16)), (notes, back)
    )
    received = lax.ppermute(give, "tp", FAR)
    expert_out = run(last_kernel, (((tokens, share), bf16),), (keep, received))
    return (mixer_out, expert_out)


def solution(mesh):
    split = Mesh(mesh.devices.reshape(8, 4, 2, mesh.shape["tp"]), EP_TP)
    placed = (
        P(EP, None),
        P(),
        P(None, "tp"),
        P(None, "tp"),
        P(None, "tp"),
        P("tp", EP),
        P("tp", EP),
        P(),
        P("tp", None),
        P(EP, None),
        P(),
        P(),
        P(),
        P(EP, None),
        P(EP, None, "tp"),
        P(EP, None, "tp"),
        P(EP, "tp", None),
    )

    return jax.shard_map(
        shards,
        mesh=split,
        in_specs=placed,
        out_specs=(P(EP_TP, None), P(EP, "tp")),
        check_vma=False,
    )
```

```python
import jax
import jax.numpy as jnp
from jax import lax
from jax.experimental import pallas as pl
from jax.experimental.pallas import tpu as pltpu
from jax.sharding import Mesh
from jax.sharding import PartitionSpec as P

EP = ("z", "y", "c")
EP_TP = ("z", "y", "c", "tp")
ZY = ("z", "y")
YC = ("y", "c")
NEAR = [(i, i ^ 1) for i in range(4)]
FAR = [(i, 3 - i) for i in range(4)]
ACROSS = [(i, i ^ 2) for i in range(4)]
SWAP = [(0, 1), (1, 0)]
CROSS = [(c * 4 + t, (c if t < 2 else 1 - c) * 4 + t) for c in range(2) for t in range(4)]
LINES = 136
CHUNKS = 2
f32 = jnp.float32
bf16 = jnp.bfloat16

epsilon = 1e-06
highest = lax.Precision.HIGHEST
floor_log = -1e30


def normalized(matrix):
    return matrix * lax.rsqrt(jnp.mean(matrix * matrix, axis=-1, keepdims=True) + epsilon)


def thirds(x):
    high = x.astype(bf16)
    rest = x - high.astype(f32)
    middle = rest.astype(bf16)
    return high, middle, (rest - middle.astype(f32)).astype(bf16)


def merged(earlier, later):
    moved = later[2] + earlier[1]
    peak = jnp.maximum(moved, later[1])
    memory = jnp.exp(moved - peak) * earlier[0] + jnp.exp(later[1] - peak) * later[0]
    return (memory, peak, earlier[2] + later[2])


def summary_at(ref, base):
    return (ref[base : base + 128, :], ref[base + 128 : base + 129, :], ref[base + 129 : base + 130, :])


def put_summary(ref, base, summary):
    row = lax.broadcasted_iota(jnp.int32, (8, 128), 0)
    ref[base : base + 128, :] = summary[0]
    ref[base + 128 : base + 136, :] = jnp.where(
        row == 0, summary[1], jnp.where(row == 1, summary[2], 0.0)
    )


def no_summary():
    return (jnp.zeros((128, 128), f32), jnp.full((1, 128), floor_log, f32), jnp.zeros((1, 128), f32))


def chosen_summary(flag, a, b):
    return tuple(jnp.where(flag, p, q) for p, q in zip(a, b))


def gate_sums(log_forget, input_gate):
    s = lax.broadcasted_iota(jnp.int32, (128, 128), 0)
    t = lax.broadcasted_iota(jnp.int32, (128, 128), 1)
    upto = (s <= t).astype(f32)
    sums = jnp.dot(log_forget[...], upto, preferred_element_type=f32, precision=highest)
    total = jnp.sum(log_forget[...], axis=1, keepdims=True)
    log_weight = total - sums + input_gate[...]
    peak = jnp.max(log_weight, axis=1, keepdims=True)
    return sums, total, log_weight, peak


def as_columns(rows):
    return jnp.concatenate([rows, jnp.zeros((120, 128), f32)], axis=0).T


def mixer_head_kernel(rows, gain, wq, wk, wv, log_forget, input_gate, q, k, v, memories, spread, normed):
    normed[...] = (normalized(rows[...].astype(f32)) * gain[...]).astype(bf16)
    for weight, target in ((wq, q), (wk, k), (wv, v)):
        target[...] = jnp.dot(normed[...], weight[...], preferred_element_type=f32).astype(bf16)
    _, total, log_weight, peak = gate_sums(log_forget, input_gate)
    columns = as_columns(jnp.exp(log_weight - peak))
    for h in range(2):
        whole_summary = None
        for b in range(4):
            n = h * 4 + b
            at = (slice(b * 128, b * 128 + 128), slice(h * 128, h * 128 + 128))
            keys = k[at].astype(f32).T.astype(bf16)
            weighted = v[at].astype(f32) * columns[:, n : n + 1]
            parts = [jnp.dot(keys, p, preferred_element_type=f32) for p in thirds(weighted)]
            memory = (parts[2] + parts[1] + parts[0]) * 128**-0.5
            memories[n * 128 : n * 128 + 128, :] = memory
            ones = jnp.ones((1, 128), f32)
            summary = (memory, peak[n : n + 1, :] * ones, total[n : n + 1, :] * ones)
            whole_summary = summary if b == 0 else merged(whole_summary, summary)
        for y in range(4):
            put_summary(spread, (2 * y + h) * LINES, whole_summary)


def fold_slab_kernel(place, members, spread, before):
    running = no_summary()
    captured = [no_summary(), no_summary()]
    for n in range(8):
        captured[n % 2] = chosen_summary(place[3] == n // 2, running, captured[n % 2])
        running = merged(running, summary_at(members, n * LINES))
    for n in range(8):
        put_summary(spread, n * LINES, running)
    for n in range(2):
        put_summary(before, n * LINES, captured[n])


def fold_all_kernel(place, slabs, before, mine, theirs):
    running = no_summary()
    start = no_summary()
    for n in range(8):
        start = chosen_summary(place[2] == n, running, start)
        if n < 7:
            running = merged(running, summary_at(slabs, n * LINES))
    pair = [merged(start, summary_at(before, n * LINES)) for n in range(2)]
    put_summary(mine, 0, chosen_summary(place[1] == 0, pair[0], pair[1]))
    put_summary(theirs, 0, chosen_summary(place[1] == 0, pair[1], pair[0]))


def mixer_tail_kernel(
    place, q, k, v, log_forget, input_gate, memories, mine, theirs, gain, weight,
    own, near, far, across_near, across_far, cells
):
    sums, total, _, peak = gate_sums(log_forget, input_gate)
    columns = as_columns(sums)
    later = lax.broadcasted_iota(jnp.int32, (128, 128), 1) > lax.broadcasted_iota(
        jnp.int32, (128, 128), 0
    )
    ones = jnp.ones((1, 128), f32)
    for h in range(2):
        state = chosen_summary(place[1] == h, summary_at(mine, 0), summary_at(theirs, 0))
        head_gain = gain[:, pl.ds(pl.multiple_of(place[0] * 256 + h * 128, 128), 128)]
        for b in range(4):
            n = h * 4 + b
            at = (slice(b * 128, b * 128 + 128), slice(h * 128, h * 128 + 128))
            column = columns[:, n : n + 1]
            within = column - sums[n : n + 1, :] + input_gate[n : n + 1, :]
            within = jnp.where(later, floor_log, within)
            carried = column + state[1][:, 0:1]
            top = jnp.maximum(jnp.max(within, axis=1, keepdims=True), carried)
            raw = lax.dot_general(
                q[at], k[at], (((1,), (1,)), ((), ())), preferred_element_type=f32
            )
            scores = raw * 128**-0.5 * jnp.exp(within - top)
            scores = jnp.where(later, 0.0, scores).astype(bf16)
            inside = jnp.dot(scores, v[at], preferred_element_type=f32)
            parts = [jnp.dot(q[at], p, preferred_element_type=f32) for p in thirds(state[0])]
            outside = parts[2] + parts[1] + parts[0]
            cell = inside + jnp.exp(carried - top) * outside
            cells[at] = (normalized(cell) * head_gain).astype(bf16)
            if b < 3:
                block = (memories[n * 128 : n * 128 + 128, :], peak[n : n + 1, :] * ones, total[n : n + 1, :] * ones)
                state = merged(state, block)
    count = own.shape[0]
    rank = place[0]
    for target, device, start in (
        (own, rank, 0),
        (near, rank ^ 1, 0),
        (far, 3 - rank, 0),
        (across_near, rank ^ 2, 0),
        (across_far, rank ^ 2, count // 2),
    ):
        at = pl.ds(pl.multiple_of(device * count + start, count // 2), target.shape[0])
        target[...] = jnp.dot(cells[at, :], weight[...], preferred_element_type=f32).astype(bf16)


def relay_kernel(near, far, from_near, from_far, to_near, to_far):
    half = from_near.shape[0]
    to_far[:half, :] = (far[:half, :].astype(f32) + from_near[...].astype(f32)).astype(bf16)
    to_far[half:, :] = far[half:, :]
    to_near[:half, :] = near[:half, :]
    to_near[half:, :] = (near[half:, :].astype(f32) + from_far[...].astype(f32)).astype(bf16)


def sum_kernel(own, near, far, out):
    total = own[...].astype(f32) + near[...].astype(f32) + far[...].astype(f32)
    out[...] = total.astype(bf16)


def cut_kernel(place, weights, own, near, far, across):
    rank = place[0]
    share = weights.shape[1] // 4
    for target, device in ((own, rank), (near, rank ^ 1), (far, 3 - rank), (across, rank ^ 2)):
        for j, quarter in enumerate((device, 3 - device)):
            target[:, j * share : (j + 1) * share] = weights[
                :, pl.ds(pl.multiple_of(quarter * share, share), share)
            ]


def dispatch_kernel(place, rows, gain, group_router, expert_router, routes, *rest):
    sends, (notes, normed) = rest[:CHUNKS], rest[CHUNKS:]
    rank, core = place[0], place[1]
    normed[...] = (normalized(rows[...].astype(f32)) * gain[...]).astype(bf16)

    def logits(weights):
        return lax.dot_general(
            weights[...], normed[...], (((1,), (1,)), ((), ())), preferred_element_type=f32
        )

    group_logits, expert_logits = logits(group_router), logits(expert_router)
    experts, tokens = expert_logits.shape
    groups = group_logits.shape[0]
    expert_ids = lax.broadcasted_iota(jnp.int32, (experts, tokens), 0)
    group_ids = lax.broadcasted_iota(jnp.int32, (groups, tokens), 0)
    named = [routes[k : k + 1, :] for k in range(2)]
    hot = [(expert_ids == e).astype(f32) for e in named]
    above = (
        lax.broadcasted_iota(jnp.int32, (tokens, tokens), 0)
        < lax.broadcasted_iota(jnp.int32, (tokens, tokens), 1)
    ).astype(bf16)
    counts = [jnp.dot(h.astype(bf16), above, preferred_element_type=f32) for h in hot]
    counts[1] = counts[1] + jnp.sum(hot[0], axis=1, keepdims=True)
    slots = []
    for k in range(2):
        at = jnp.sum(hot[k] * counts[k], axis=0, keepdims=True).astype(jnp.int32)
        here = ((named[k] & 1) ^ core) == rank // 2
        slots.append(jnp.where(here, (named[k] >> 1) * 16 + at, -1))
    chosen = [jnp.sum(h * expert_logits, axis=0, keepdims=True) for h in hot]
    grouped = [
        jnp.sum(jnp.where(group_ids == e // (experts // groups), group_logits, 0.0), axis=0, keepdims=True)
        for e in named
    ]
    combine = [
        jax.nn.sigmoid(grouped[k]) * jax.nn.sigmoid(chosen[k] - chosen[1 - k]) for k in range(2)
    ]
    share = rows.shape[1] // 4
    count = sends[0].shape[0]
    each = 16 // CHUNKS
    slot_ids = lax.broadcasted_iota(jnp.int32, (count, tokens), 0)
    for n, send in enumerate(sends):
        ids = (slot_ids // each) * 16 + slot_ids % each + n * each
        pick = ((ids == slots[0]) | (ids == slots[1])).astype(bf16)
        for j, quarter in enumerate((rank, 3 - rank)):
            features = normed[:, pl.ds(pl.multiple_of(quarter * share, share), share)]
            send[:, j * share : (j + 1) * share] = jnp.dot(
                pick, features, preferred_element_type=f32
            ).astype(bf16)
    row = lax.broadcasted_iota(jnp.int32, (128, tokens), 0)
    wide = jnp.where(row == 0, slots[0].astype(f32), slots[1].astype(f32))
    notes[...] = jnp.where(row < 2, wide, jnp.where(row == 2, combine[0], combine[1])).T


def hidden_kernel(place, own, other, gate, up, far_gate, far_up, out, sums):
    share = own.shape[1] // 2
    units = gate.shape[1]
    step = pl.program_id(0)
    for n, rows in enumerate((own, own, other, other)):

        @pl.when(step == n)
        def _():
            features = rows[:, (n % 2) * share : (n % 2 + 1) * share]
            for j, weight in enumerate((gate, far_gate, up, far_up)):
                at = slice(j * units, (j + 1) * units)
                term = jnp.dot(features, weight[...], preferred_element_type=f32)
                sums[:, at] = term if n == 0 else sums[:, at] + term

    @pl.when(step == 3)
    def _():
        out[...] = (jax.nn.silu(sums[:, : 2 * units]) * sums[:, 2 * units :]).astype(bf16)


def hidden_of(place, own, other, weights):
    share = own.shape[1] // 2
    units = weights[0].shape[1]
    rows = pl.BlockSpec(own.shape, lambda n, place: (0, 0))

    def block(n, place):
        device = place[0] ^ (n // 2)
        return (jnp.where(n % 2 == 0, device, 3 - device), 0)

    return pl.pallas_call(
        hidden_kernel,
        out_shape=jax.ShapeDtypeStruct((own.shape[0], 2 * units), bf16),
        grid_spec=pltpu.PrefetchScalarGridSpec(
            num_scalar_prefetch=1,
            grid=(4,),
            in_specs=[rows, rows] + [pl.BlockSpec((share, units), block)] * 4,
            out_specs=pl.BlockSpec((own.shape[0], 2 * units), lambda n, place: (0, 0)),
            scratch_shapes=[pltpu.VMEM((own.shape[0], 4 * units), f32)],
        ),
        compiler_params=pltpu.CompilerParams(
            vmem_limit_bytes=32 * 1024 * 1024, dimension_semantics=("arbitrary",)
        ),
    )(place, own, other, *weights)


def down_kernel(*refs):
    pairs, (w_own, w_far, w_near, w_across, out) = refs[: 2 * CHUNKS], refs[2 * CHUNKS :]
    each = 16 // CHUNKS
    for n in range(CHUNKS):
        own, other = pairs[2 * n : 2 * n + 2]
        units = own.shape[1] // 2
        total = jnp.dot(own[:, :units], w_own[...], preferred_element_type=f32)
        total = total + jnp.dot(own[:, units:], w_far[...], preferred_element_type=f32)
        total = total + jnp.dot(other[:, :units], w_near[...], preferred_element_type=f32)
        total = total + jnp.dot(other[:, units:], w_across[...], preferred_element_type=f32)
        out[:, n * each : (n + 1) * each, :] = total.astype(bf16).reshape(
            out.shape[0], each, out.shape[2]
        )


def combine_kernel(notes, rows, keep, send):
    tokens, share = keep.shape
    slots = [notes[:, k : k + 1].astype(jnp.int32) for k in range(2)]
    lanes = lax.broadcasted_iota(jnp.int32, (tokens, rows.shape[0]), 1)
    weight = jnp.where(lanes == slots[0], notes[:, 2:3], 0.0) + jnp.where(
        lanes == slots[1], notes[:, 3:4], 0.0
    )
    high = weight.astype(bf16)
    low = (weight - high.astype(f32)).astype(bf16)
    total = jnp.dot(high, rows[...], preferred_element_type=f32)
    total = total + jnp.dot(low, rows[...], preferred_element_type=f32)
    keep[...] = total[:, :share]
    send[...] = total[:, share:].astype(bf16)


def last_kernel(keep, received, out):
    out[...] = (keep[...] + received[...].astype(f32)).astype(bf16)


def run(kernel, shapes, args, place=None, scratch=()):
    specs = [pl.BlockSpec(memory_space=pltpu.VMEM)] * len(args)
    if place is not None:
        specs = [pl.BlockSpec(memory_space=pltpu.SMEM)] + specs
        args = (place, *args)
    outs = tuple(jax.ShapeDtypeStruct(s, d) for s, d in shapes)
    result = pl.pallas_call(
        kernel,
        out_shape=outs,
        in_specs=specs,
        out_specs=tuple([pl.BlockSpec(memory_space=pltpu.VMEM)] * len(outs)),
        scratch_shapes=[pltpu.VMEM(s, d) for s, d in scratch],
        compiler_params=pltpu.CompilerParams(vmem_limit_bytes=48 * 1024 * 1024),
    )(*args)
    return result if len(outs) > 1 else result[0]


def traded(x, axis):
    return lax.all_to_all(x, axis, 0, 0, tiled=True)


def shards(
    mixer_in,
    mixer_gain,
    query_weight,
    key_weight,
    value_weight,
    input_gate,
    forget_gate,
    head_gain,
    mixer_out_weight,
    expert_in,
    expert_gain,
    group_router,
    expert_router,
    routes,
    gate_experts,
    up_experts,
    down_experts,
):
    place = jnp.stack([lax.axis_index(a) for a in ("tp", "c", "z", "y")]).astype(jnp.int32)
    tokens, width = expert_in.shape
    share = width // 4
    slots = 32 * 16
    gate, up, down = gate_experts[0], up_experts[0], down_experts[0]
    units = gate.shape[1]
    far_gate = lax.ppermute(gate, "tp", FAR)
    far_up = lax.ppermute(up, "tp", FAR)
    *sends, notes = run(
        dispatch_kernel,
        (((slots // CHUNKS, 2 * share), bf16),) * CHUNKS + (((tokens, 128), f32),),
        (expert_in, expert_gain.reshape(1, -1), group_router.T, expert_router.T, routes.T),
        place,
        [((tokens, width), bf16)],
    )
    arrived = []
    for send in sends:
        send = lax.ppermute(send, ("c", "tp"), CROSS)
        arrived.append(traded(send, ZY))

    w_own, w_near, w_far, w_across = run(
        cut_kernel, (((units, 2 * share), bf16),) * 4, (down,), place
    )
    w_near = lax.ppermute(w_near, "tp", NEAR)
    w_far = lax.ppermute(w_far, "tp", FAR)
    w_across = lax.ppermute(w_across, "tp", ACROSS)

    row_count = mixer_in.shape[0]
    local = query_weight.shape[1]
    log_forget = jax.nn.log_sigmoid(forget_gate).reshape(8, 128)
    inputs = input_gate.reshape(8, 128)
    q, k, v, memories, spread = run(
        mixer_head_kernel,
        (((row_count, local), bf16),) * 3 + (((8 * 128, 128), f32), ((8 * LINES, 128), f32)),
        (mixer_in, mixer_gain.reshape(1, -1), query_weight, key_weight, value_weight, log_forget, inputs),
        None,
        [((row_count, width), bf16)],
    )
    members = traded(spread, YC)
    spread, before = run(
        fold_slab_kernel, (((8 * LINES, 128), f32), ((2 * LINES, 128), f32)), (members,), place
    )
    slabs = traded(spread, "z")
    mine, theirs = run(fold_all_kernel, (((LINES, 128), f32),) * 2, (slabs, before), place)
    theirs = lax.ppermute(theirs, "c", SWAP)
    count = row_count // 4
    own, near, far, across_near, across_far = run(
        mixer_tail_kernel,
        (((count, width), bf16),) * 3 + (((count // 2, width), bf16),) * 2,
        (q, k, v, log_forget, inputs, memories, mine, theirs, head_gain.reshape(1, -1), mixer_out_weight),
        place,
        [((row_count, local), bf16)],
    )
    from_near = lax.ppermute(across_near, "tp", NEAR)
    from_far = lax.ppermute(across_far, "tp", FAR)
    to_near, to_far = run(
        relay_kernel, (((count, width), bf16),) * 2, (near, far, from_near, from_far)
    )
    near = lax.ppermute(to_near, "tp", NEAR)
    far = lax.ppermute(to_far, "tp", FAR)
    mixer_out = run(sum_kernel, (((count, width), bf16),), (own, near, far))

    pairs = []
    for rows in arrived:
        other_rows = lax.ppermute(rows, "tp", NEAR)
        hidden = hidden_of(place, rows, other_rows, (gate, up, far_gate, far_up))
        pairs += [hidden, lax.ppermute(hidden, "tp", NEAR)]
    result = run(
        down_kernel, (((32, 16, 2 * share), bf16),), (*pairs, w_own, w_far, w_near, w_across)
    )
    back = traded(result.reshape(slots, 2 * share), ZY)
    back = lax.ppermute(back, ("c", "tp"), CROSS)
    keep, give = run(
        combine_kernel, (((tokens, share), f32), ((tokens, share), bf16)), (notes, back)
    )
    received = lax.ppermute(give, "tp", FAR)
    expert_out = run(last_kernel, (((tokens, share), bf16),), (keep, received))
    return (mixer_out, expert_out)


def solution(mesh):
    split = Mesh(mesh.devices.reshape(8, 4, 2, mesh.shape["tp"]), EP_TP)
    placed = (
        P(EP, None),
        P(),
        P(None, "tp"),
        P(None, "tp"),
        P(None, "tp"),
        P("tp", EP),
        P("tp", EP),
        P(),
        P("tp", None),
        P(EP, None),
        P(),
        P(),
        P(),
        P(EP, None),
        P(EP, None, "tp"),
        P(EP, None, "tp"),
        P(EP, "tp", None),
    )

    return jax.shard_map(
        shards,
        mesh=split,
        in_specs=placed,
        out_specs=(P(EP_TP, None), P(EP, "tp")),
        check_vma=False,
    )
```

```python
import jax
import jax.numpy as jnp
from jax import lax
from jax.experimental import pallas as pl
from jax.experimental.pallas import tpu as pltpu
from jax.sharding import Mesh
from jax.sharding import PartitionSpec as P

EP = ("z", "y", "c")
EP_TP = ("z", "y", "c", "tp")
ZY = ("z", "y")
YC = ("y", "c")
NEAR = [(i, i ^ 1) for i in range(4)]
FAR = [(i, 3 - i) for i in range(4)]
SWAP = [(0, 1), (1, 0)]
CROSS = [(c * 4 + t, (c if t < 2 else 1 - c) * 4 + t) for c in range(2) for t in range(4)]
LINES = 136
CHUNKS = 1
f32 = jnp.float32
bf16 = jnp.bfloat16

epsilon = 1e-06
highest = lax.Precision.HIGHEST
floor_log = -1e30


def normalized(matrix):
    return matrix * lax.rsqrt(jnp.mean(matrix * matrix, axis=-1, keepdims=True) + epsilon)


def thirds(x):
    high = x.astype(bf16)
    rest = x - high.astype(f32)
    middle = rest.astype(bf16)
    return high, middle, (rest - middle.astype(f32)).astype(bf16)


def merged(earlier, later):
    moved = later[2] + earlier[1]
    peak = jnp.maximum(moved, later[1])
    memory = jnp.exp(moved - peak) * earlier[0] + jnp.exp(later[1] - peak) * later[0]
    return (memory, peak, earlier[2] + later[2])


def summary_at(ref, base):
    return (ref[base : base + 128, :], ref[base + 128 : base + 129, :], ref[base + 129 : base + 130, :])


def put_summary(ref, base, summary):
    row = lax.broadcasted_iota(jnp.int32, (8, 128), 0)
    ref[base : base + 128, :] = summary[0]
    ref[base + 128 : base + 136, :] = jnp.where(
        row == 0, summary[1], jnp.where(row == 1, summary[2], 0.0)
    )


def no_summary():
    return (jnp.zeros((128, 128), f32), jnp.full((1, 128), floor_log, f32), jnp.zeros((1, 128), f32))


def chosen_summary(flag, a, b):
    return tuple(jnp.where(flag, p, q) for p, q in zip(a, b))


def gate_sums(log_forget, input_gate):
    s = lax.broadcasted_iota(jnp.int32, (128, 128), 0)
    t = lax.broadcasted_iota(jnp.int32, (128, 128), 1)
    upto = (s <= t).astype(f32)
    sums = jnp.dot(log_forget[...], upto, preferred_element_type=f32, precision=highest)
    total = jnp.sum(log_forget[...], axis=1, keepdims=True)
    log_weight = total - sums + input_gate[...]
    peak = jnp.max(log_weight, axis=1, keepdims=True)
    return sums, total, log_weight, peak


def as_columns(rows):
    return jnp.concatenate([rows, jnp.zeros((120, 128), f32)], axis=0).T


def mixer_head_kernel(rows, gain, wq, wk, wv, log_forget, input_gate, q, k, v, memories, spread, normed):
    normed[...] = (normalized(rows[...].astype(f32)) * gain[...]).astype(bf16)
    for weight, target in ((wq, q), (wk, k), (wv, v)):
        target[...] = jnp.dot(normed[...], weight[...], preferred_element_type=f32).astype(bf16)
    _, total, log_weight, peak = gate_sums(log_forget, input_gate)
    columns = as_columns(jnp.exp(log_weight - peak))
    for h in range(2):
        whole_summary = None
        for b in range(4):
            n = h * 4 + b
            at = (slice(b * 128, b * 128 + 128), slice(h * 128, h * 128 + 128))
            keys = k[at].astype(f32).T.astype(bf16)
            weighted = v[at].astype(f32) * columns[:, n : n + 1]
            parts = [jnp.dot(keys, p, preferred_element_type=f32) for p in thirds(weighted)]
            memory = (parts[2] + parts[1] + parts[0]) * 128**-0.5
            memories[n * 128 : n * 128 + 128, :] = memory
            ones = jnp.ones((1, 128), f32)
            summary = (memory, peak[n : n + 1, :] * ones, total[n : n + 1, :] * ones)
            whole_summary = summary if b == 0 else merged(whole_summary, summary)
        for y in range(4):
            put_summary(spread, (2 * y + h) * LINES, whole_summary)


def fold_slab_kernel(place, members, spread, before):
    running = no_summary()
    captured = [no_summary(), no_summary()]
    for n in range(8):
        captured[n % 2] = chosen_summary(place[3] == n // 2, running, captured[n % 2])
        running = merged(running, summary_at(members, n * LINES))
    for n in range(8):
        put_summary(spread, n * LINES, running)
    for n in range(2):
        put_summary(before, n * LINES, captured[n])


def fold_all_kernel(place, slabs, before, mine, theirs):
    running = no_summary()
    start = no_summary()
    for n in range(8):
        start = chosen_summary(place[2] == n, running, start)
        if n < 7:
            running = merged(running, summary_at(slabs, n * LINES))
    pair = [merged(start, summary_at(before, n * LINES)) for n in range(2)]
    put_summary(mine, 0, chosen_summary(place[1] == 0, pair[0], pair[1]))
    put_summary(theirs, 0, chosen_summary(place[1] == 0, pair[1], pair[0]))


def mixer_tail_kernel(
    place, q, k, v, log_forget, input_gate, memories, mine, theirs, gain, weight,
    own, near, far, across_near, across_far, cells
):
    sums, total, _, peak = gate_sums(log_forget, input_gate)
    columns = as_columns(sums)
    later = lax.broadcasted_iota(jnp.int32, (128, 128), 1) > lax.broadcasted_iota(
        jnp.int32, (128, 128), 0
    )
    ones = jnp.ones((1, 128), f32)
    for h in range(2):
        state = chosen_summary(place[1] == h, summary_at(mine, 0), summary_at(theirs, 0))
        head_gain = gain[:, pl.ds(pl.multiple_of(place[0] * 256 + h * 128, 128), 128)]
        for b in range(4):
            n = h * 4 + b
            at = (slice(b * 128, b * 128 + 128), slice(h * 128, h * 128 + 128))
            column = columns[:, n : n + 1]
            within = column - sums[n : n + 1, :] + input_gate[n : n + 1, :]
            within = jnp.where(later, floor_log, within)
            carried = column + state[1][:, 0:1]
            top = jnp.maximum(jnp.max(within, axis=1, keepdims=True), carried)
            raw = lax.dot_general(
                q[at], k[at], (((1,), (1,)), ((), ())), preferred_element_type=f32
            )
            scores = raw * 128**-0.5 * jnp.exp(within - top)
            scores = jnp.where(later, 0.0, scores).astype(bf16)
            inside = jnp.dot(scores, v[at], preferred_element_type=f32)
            parts = [jnp.dot(q[at], p, preferred_element_type=f32) for p in thirds(state[0])]
            outside = parts[2] + parts[1] + parts[0]
            cell = inside + jnp.exp(carried - top) * outside
            cells[at] = (normalized(cell) * head_gain).astype(bf16)
            if b < 3:
                block = (memories[n * 128 : n * 128 + 128, :], peak[n : n + 1, :] * ones, total[n : n + 1, :] * ones)
                state = merged(state, block)
    count = own.shape[0]
    rank = place[0]
    for target, device, start in (
        (own, rank, 0),
        (near, rank ^ 1, 0),
        (far, 3 - rank, 0),
        (across_near, rank ^ 2, 0),
        (across_far, rank ^ 2, count // 2),
    ):
        at = pl.ds(pl.multiple_of(device * count + start, count // 2), target.shape[0])
        target[...] = jnp.dot(cells[at, :], weight[...], preferred_element_type=f32).astype(bf16)


def relay_kernel(near, far, from_near, from_far, to_near, to_far):
    half = from_near.shape[0]
    to_far[:half, :] = (far[:half, :].astype(f32) + from_near[...].astype(f32)).astype(bf16)
    to_far[half:, :] = far[half:, :]
    to_near[:half, :] = near[:half, :]
    to_near[half:, :] = (near[half:, :].astype(f32) + from_far[...].astype(f32)).astype(bf16)


def sum_kernel(own, near, far, out):
    total = own[...].astype(f32) + near[...].astype(f32) + far[...].astype(f32)
    out[...] = total.astype(bf16)


def cut_kernel(place, weights, far_weights, keep, give):
    rank = place[0]
    units = weights.shape[0]
    share = weights.shape[1] // 4
    for target, device in ((keep, rank), (give, rank ^ 1)):
        for j, quarter in enumerate((device, 3 - device)):
            at = pl.ds(pl.multiple_of(quarter * share, share), share)
            columns = slice(j * share, (j + 1) * share)
            target[:units, columns] = weights[:, at]
            target[units:, columns] = far_weights[:, at]


def dispatch_kernel(place, rows, gain, group_router, expert_router, routes, *rest):
    sends, (notes, normed) = rest[:CHUNKS], rest[CHUNKS:]
    rank, core = place[0], place[1]
    normed[...] = (normalized(rows[...].astype(f32)) * gain[...]).astype(bf16)

    def logits(weights):
        return lax.dot_general(
            weights[...], normed[...], (((1,), (1,)), ((), ())), preferred_element_type=f32
        )

    group_logits, expert_logits = logits(group_router), logits(expert_router)
    experts, tokens = expert_logits.shape
    groups = group_logits.shape[0]
    expert_ids = lax.broadcasted_iota(jnp.int32, (experts, tokens), 0)
    group_ids = lax.broadcasted_iota(jnp.int32, (groups, tokens), 0)
    named = [routes[k : k + 1, :] for k in range(2)]
    hot = [(expert_ids == e).astype(f32) for e in named]
    above = (
        lax.broadcasted_iota(jnp.int32, (tokens, tokens), 0)
        < lax.broadcasted_iota(jnp.int32, (tokens, tokens), 1)
    ).astype(bf16)
    counts = [jnp.dot(h.astype(bf16), above, preferred_element_type=f32) for h in hot]
    counts[1] = counts[1] + jnp.sum(hot[0], axis=1, keepdims=True)
    slots = []
    for k in range(2):
        at = jnp.sum(hot[k] * counts[k], axis=0, keepdims=True).astype(jnp.int32)
        here = ((named[k] & 1) ^ core) == rank // 2
        slots.append(jnp.where(here, (named[k] >> 1) * 16 + at, -1))
    chosen = [jnp.sum(h * expert_logits, axis=0, keepdims=True) for h in hot]
    grouped = [
        jnp.sum(jnp.where(group_ids == e // (experts // groups), group_logits, 0.0), axis=0, keepdims=True)
        for e in named
    ]
    combine = [
        jax.nn.sigmoid(grouped[k]) * jax.nn.sigmoid(chosen[k] - chosen[1 - k]) for k in range(2)
    ]
    share = rows.shape[1] // 4
    count = sends[0].shape[0]
    each = 16 // CHUNKS
    slot_ids = lax.broadcasted_iota(jnp.int32, (count, tokens), 0)
    for n, send in enumerate(sends):
        ids = (slot_ids // each) * 16 + slot_ids % each + n * each
        pick = ((ids == slots[0]) | (ids == slots[1])).astype(bf16)
        for j, quarter in enumerate((rank, 3 - rank)):
            features = normed[:, pl.ds(pl.multiple_of(quarter * share, share), share)]
            send[:, j * share : (j + 1) * share] = jnp.dot(
                pick, features, preferred_element_type=f32
            ).astype(bf16)
    row = lax.broadcasted_iota(jnp.int32, (128, tokens), 0)
    wide = jnp.where(row == 0, slots[0].astype(f32), slots[1].astype(f32))
    notes[...] = jnp.where(row < 2, wide, jnp.where(row == 2, combine[0], combine[1])).T


def hidden_kernel(place, own, other, gate, up, far_gate, far_up, out, sums):
    share = own.shape[1] // 2
    units = gate.shape[1]
    step = pl.program_id(0)
    for n, rows in enumerate((own, own, other, other)):

        @pl.when(step == n)
        def _():
            features = rows[:, (n % 2) * share : (n % 2 + 1) * share]
            for j, weight in enumerate((gate, far_gate, up, far_up)):
                at = slice(j * units, (j + 1) * units)
                term = jnp.dot(features, weight[...], preferred_element_type=f32)
                sums[:, at] = term if n == 0 else sums[:, at] + term

    @pl.when(step == 3)
    def _():
        out[...] = (jax.nn.silu(sums[:, : 2 * units]) * sums[:, 2 * units :]).astype(bf16)


def hidden_of(place, own, other, weights):
    share = own.shape[1] // 2
    units = weights[0].shape[1]
    rows = pl.BlockSpec(own.shape, lambda n, place: (0, 0))

    def block(n, place):
        device = place[0] ^ (n // 2)
        return (jnp.where(n % 2 == 0, device, 3 - device), 0)

    return pl.pallas_call(
        hidden_kernel,
        out_shape=jax.ShapeDtypeStruct((own.shape[0], 2 * units), bf16),
        grid_spec=pltpu.PrefetchScalarGridSpec(
            num_scalar_prefetch=1,
            grid=(4,),
            in_specs=[rows, rows] + [pl.BlockSpec((share, units), block)] * 4,
            out_specs=pl.BlockSpec((own.shape[0], 2 * units), lambda n, place: (0, 0)),
            scratch_shapes=[pltpu.VMEM((own.shape[0], 4 * units), f32)],
        ),
        compiler_params=pltpu.CompilerParams(
            vmem_limit_bytes=16 * 1024 * 1024, dimension_semantics=("arbitrary",)
        ),
    )(place, own, other, *weights)


def down_kernel(own, other, mine, theirs, out):
    total = jnp.dot(own[...], mine[...], preferred_element_type=f32)
    total = total + jnp.dot(other[...], theirs[...], preferred_element_type=f32)
    out[...] = total.astype(bf16)


def combine_kernel(notes, rows, keep, send):
    tokens, share = keep.shape
    slots = [notes[:, k : k + 1].astype(jnp.int32) for k in range(2)]
    lanes = lax.broadcasted_iota(jnp.int32, (tokens, rows.shape[0]), 1)
    weight = jnp.where(lanes == slots[0], notes[:, 2:3], 0.0) + jnp.where(
        lanes == slots[1], notes[:, 3:4], 0.0
    )
    high = weight.astype(bf16)
    low = (weight - high.astype(f32)).astype(bf16)
    total = jnp.dot(high, rows[...], preferred_element_type=f32)
    total = total + jnp.dot(low, rows[...], preferred_element_type=f32)
    keep[...] = total[:, :share]
    send[...] = total[:, share:].astype(bf16)


def last_kernel(keep, received, out):
    out[...] = (keep[...] + received[...].astype(f32)).astype(bf16)


def run(kernel, shapes, args, place=None, scratch=(), room=8):
    def block(shape):
        return pl.BlockSpec(tuple(shape), lambda n: (0,) * len(shape))

    specs = [block(a.shape) for a in args]
    if place is not None:
        specs = [pl.BlockSpec(memory_space=pltpu.SMEM)] + specs
        args = (place, *args)
    outs = tuple(jax.ShapeDtypeStruct(s, d) for s, d in shapes)
    result = pl.pallas_call(
        kernel,
        out_shape=outs,
        grid=(1,),
        in_specs=specs,
        out_specs=tuple(block(o.shape) for o in outs),
        scratch_shapes=[pltpu.VMEM(s, d) for s, d in scratch],
        compiler_params=pltpu.CompilerParams(vmem_limit_bytes=room * 1024 * 1024),
    )(*args)
    return result if len(outs) > 1 else result[0]


def traded(x, axis):
    return lax.all_to_all(x, axis, 0, 0, tiled=True)


def shards(
    mixer_in,
    mixer_gain,
    query_weight,
    key_weight,
    value_weight,
    input_gate,
    forget_gate,
    head_gain,
    mixer_out_weight,
    expert_in,
    expert_gain,
    group_router,
    expert_router,
    routes,
    gate_experts,
    up_experts,
    down_experts,
):
    place = jnp.stack([lax.axis_index(a) for a in ("tp", "c", "z", "y")]).astype(jnp.int32)
    tokens, width = expert_in.shape
    share = width // 4
    slots = 32 * 16
    gate, up, down = gate_experts[0], up_experts[0], down_experts[0]
    units = gate.shape[1]
    far_down = lax.ppermute(down, "tp", FAR)
    far_gate = lax.ppermute(gate, "tp", FAR)
    far_up = lax.ppermute(up, "tp", FAR)
    *sends, notes = run(
        dispatch_kernel,
        (((slots // CHUNKS, 2 * share), bf16),) * CHUNKS + (((tokens, 128), f32),),
        (expert_in, expert_gain.reshape(1, -1), group_router.T, expert_router.T, routes.T),
        place,
        [((tokens, width), bf16)],
        room=16,
    )
    arrived = []
    for send in sends:
        send = lax.ppermute(send, ("c", "tp"), CROSS)
        arrived.append(traded(send, ZY))

    down_mine, give = run(
        cut_kernel, (((2 * units, 2 * share), bf16),) * 2, (down, far_down), place, room=16
    )
    down_theirs = lax.ppermute(give, "tp", NEAR)

    row_count = mixer_in.shape[0]
    local = query_weight.shape[1]
    log_forget = jax.nn.log_sigmoid(forget_gate).reshape(8, 128)
    inputs = input_gate.reshape(8, 128)
    q, k, v, memories, spread = run(
        mixer_head_kernel,
        (((row_count, local), bf16),) * 3 + (((8 * 128, 128), f32), ((8 * LINES, 128), f32)),
        (mixer_in, mixer_gain.reshape(1, -1), query_weight, key_weight, value_weight, log_forget, inputs),
        None,
        [((row_count, width), bf16)],
        room=24,
    )
    members = traded(spread, YC)
    spread, before = run(
        fold_slab_kernel, (((8 * LINES, 128), f32), ((2 * LINES, 128), f32)), (members,), place
    )
    slabs = traded(spread, "z")
    mine, theirs = run(fold_all_kernel, (((LINES, 128), f32),) * 2, (slabs, before), place)
    theirs = lax.ppermute(theirs, "c", SWAP)
    count = row_count // 4
    own, near, far, across_near, across_far = run(
        mixer_tail_kernel,
        (((count, width), bf16),) * 3 + (((count // 2, width), bf16),) * 2,
        (q, k, v, log_forget, inputs, memories, mine, theirs, head_gain.reshape(1, -1), mixer_out_weight),
        place,
        [((row_count, local), bf16)],
        room=16,
    )
    from_near = lax.ppermute(across_near, "tp", NEAR)
    from_far = lax.ppermute(across_far, "tp", FAR)
    to_near, to_far = run(
        relay_kernel, (((count, width), bf16),) * 2, (near, far, from_near, from_far)
    )
    near = lax.ppermute(to_near, "tp", NEAR)
    far = lax.ppermute(to_far, "tp", FAR)
    mixer_out = run(sum_kernel, (((count, width), bf16),), (own, near, far))

    pairs = []
    for rows in arrived:
        other_rows = lax.ppermute(rows, "tp", NEAR)
        hidden = hidden_of(place, rows, other_rows, (gate, up, far_gate, far_up))
        pairs += [hidden, lax.ppermute(hidden, "tp", NEAR)]
    result = run(
        down_kernel, (((slots, 2 * share), bf16),), (*pairs, down_mine, down_theirs), room=16
    )
    back = traded(result, ZY)
    back = lax.ppermute(back, ("c", "tp"), CROSS)
    keep, give = run(
        combine_kernel, (((tokens, share), f32), ((tokens, share), bf16)), (notes, back)
    )
    received = lax.ppermute(give, "tp", FAR)
    expert_out = run(last_kernel, (((tokens, share), bf16),), (keep, received))
    return (mixer_out, expert_out)


def solution(mesh):
    split = Mesh(mesh.devices.reshape(8, 4, 2, mesh.shape["tp"]), EP_TP)
    placed = (
        P(EP, None),
        P(),
        P(None, "tp"),
        P(None, "tp"),
        P(None, "tp"),
        P("tp", EP),
        P("tp", EP),
        P(),
        P("tp", None),
        P(EP, None),
        P(),
        P(),
        P(),
        P(EP, None),
        P(EP, None, "tp"),
        P(EP, None, "tp"),
        P(EP, "tp", None),
    )

    return jax.shard_map(
        shards,
        mesh=split,
        in_specs=placed,
        out_specs=(P(EP_TP, None), P(EP, "tp")),
        check_vma=False,
    )
```

```python
import jax
import jax.numpy as jnp
from jax import lax
from jax.experimental import pallas as pl
from jax.experimental.pallas import tpu as pltpu
from jax.sharding import Mesh
from jax.sharding import PartitionSpec as P

EP = ("z", "y", "c")
EP_TP = ("z", "y", "c", "tp")
ZY = ("z", "y")
YC = ("y", "c")
NEAR = [(i, i ^ 1) for i in range(4)]
FAR = [(i, 3 - i) for i in range(4)]
SWAP = [(0, 1), (1, 0)]
CROSS = [(c * 4 + t, (c if t < 2 else 1 - c) * 4 + t) for c in range(2) for t in range(4)]
LAST = [(c * 4 + t, (c if t < 2 else 1 - c) * 4 + 3 - t) for c in range(2) for t in range(4)]
LINES = 136
f32 = jnp.float32
bf16 = jnp.bfloat16

epsilon = 1e-06
highest = lax.Precision.HIGHEST
floor_log = -1e30


def normalized(matrix):
    return matrix * lax.rsqrt(jnp.mean(matrix * matrix, axis=-1, keepdims=True) + epsilon)


def thirds(x):
    high = x.astype(bf16)
    rest = x - high.astype(f32)
    middle = rest.astype(bf16)
    return high, middle, (rest - middle.astype(f32)).astype(bf16)


def merged(earlier, later):
    moved = later[2] + earlier[1]
    peak = jnp.maximum(moved, later[1])
    memory = jnp.exp(moved - peak) * earlier[0] + jnp.exp(later[1] - peak) * later[0]
    return (memory, peak, earlier[2] + later[2])


def summary_at(ref, base):
    return (ref[base : base + 128, :], ref[base + 128 : base + 129, :], ref[base + 129 : base + 130, :])


def put_summary(ref, base, summary):
    row = lax.broadcasted_iota(jnp.int32, (8, 128), 0)
    ref[base : base + 128, :] = summary[0]
    ref[base + 128 : base + 136, :] = jnp.where(
        row == 0, summary[1], jnp.where(row == 1, summary[2], 0.0)
    )


def no_summary():
    return (jnp.zeros((128, 128), f32), jnp.full((1, 128), floor_log, f32), jnp.zeros((1, 128), f32))


def chosen_summary(flag, a, b):
    return tuple(jnp.where(flag, p, q) for p, q in zip(a, b))


def gate_sums(log_forget, input_gate):
    s = lax.broadcasted_iota(jnp.int32, (128, 128), 0)
    t = lax.broadcasted_iota(jnp.int32, (128, 128), 1)
    upto = (s <= t).astype(f32)
    sums = jnp.dot(log_forget[...], upto, preferred_element_type=f32, precision=highest)
    total = jnp.sum(log_forget[...], axis=1, keepdims=True)
    log_weight = total - sums + input_gate[...]
    peak = jnp.max(log_weight, axis=1, keepdims=True)
    return sums, total, log_weight, peak


def as_columns(rows):
    return jnp.concatenate([rows, jnp.zeros((120, 128), f32)], axis=0).T


def mixer_head_kernel(rows, gain, wq, wk, wv, log_forget, input_gate, q, k, v, memories, spread, normed):
    normed[...] = (normalized(rows[...].astype(f32)) * gain[...]).astype(bf16)
    for weight, target in ((wq, q), (wk, k), (wv, v)):
        target[...] = jnp.dot(normed[...], weight[...], preferred_element_type=f32).astype(bf16)
    _, total, log_weight, peak = gate_sums(log_forget, input_gate)
    columns = as_columns(jnp.exp(log_weight - peak))
    for h in range(2):
        whole_summary = None
        for b in range(4):
            n = h * 4 + b
            at = (slice(b * 128, b * 128 + 128), slice(h * 128, h * 128 + 128))
            keys = k[at].astype(f32).T.astype(bf16)
            weighted = v[at].astype(f32) * columns[:, n : n + 1]
            parts = [jnp.dot(keys, p, preferred_element_type=f32) for p in thirds(weighted)]
            memory = (parts[2] + parts[1] + parts[0]) * 128**-0.5
            memories[n * 128 : n * 128 + 128, :] = memory
            ones = jnp.ones((1, 128), f32)
            summary = (memory, peak[n : n + 1, :] * ones, total[n : n + 1, :] * ones)
            whole_summary = summary if b == 0 else merged(whole_summary, summary)
        for y in range(4):
            put_summary(spread, (2 * y + h) * LINES, whole_summary)


def fold_slab_kernel(place, members, spread, before):
    running = no_summary()
    captured = [no_summary(), no_summary()]
    for n in range(8):
        captured[n % 2] = chosen_summary(place[3] == n // 2, running, captured[n % 2])
        running = merged(running, summary_at(members, n * LINES))
    for n in range(8):
        put_summary(spread, n * LINES, running)
    for n in range(2):
        put_summary(before, n * LINES, captured[n])


def fold_all_kernel(place, slabs, before, mine, theirs):
    running = no_summary()
    start = no_summary()
    for n in range(8):
        start = chosen_summary(place[2] == n, running, start)
        if n < 7:
            running = merged(running, summary_at(slabs, n * LINES))
    pair = [merged(start, summary_at(before, n * LINES)) for n in range(2)]
    put_summary(mine, 0, chosen_summary(place[1] == 0, pair[0], pair[1]))
    put_summary(theirs, 0, chosen_summary(place[1] == 0, pair[1], pair[0]))


def mixer_tail_kernel(
    place, q, k, v, log_forget, input_gate, memories, mine, theirs, gain, weight,
    own, near, far, across_near, across_far, cells
):
    sums, total, _, peak = gate_sums(log_forget, input_gate)
    columns = as_columns(sums)
    later = lax.broadcasted_iota(jnp.int32, (128, 128), 1) > lax.broadcasted_iota(
        jnp.int32, (128, 128), 0
    )
    ones = jnp.ones((1, 128), f32)
    for h in range(2):
        state = chosen_summary(place[1] == h, summary_at(mine, 0), summary_at(theirs, 0))
        head_gain = gain[:, pl.ds(pl.multiple_of(place[0] * 256 + h * 128, 128), 128)]
        for b in range(4):
            n = h * 4 + b
            at = (slice(b * 128, b * 128 + 128), slice(h * 128, h * 128 + 128))
            column = columns[:, n : n + 1]
            within = column - sums[n : n + 1, :] + input_gate[n : n + 1, :]
            within = jnp.where(later, floor_log, within)
            carried = column + state[1][:, 0:1]
            top = jnp.maximum(jnp.max(within, axis=1, keepdims=True), carried)
            raw = lax.dot_general(
                q[at], k[at], (((1,), (1,)), ((), ())), preferred_element_type=f32
            )
            scores = raw * 128**-0.5 * jnp.exp(within - top)
            scores = jnp.where(later, 0.0, scores).astype(bf16)
            inside = jnp.dot(scores, v[at], preferred_element_type=f32)
            parts = [jnp.dot(q[at], p, preferred_element_type=f32) for p in thirds(state[0])]
            outside = parts[2] + parts[1] + parts[0]
            cell = inside + jnp.exp(carried - top) * outside
            cells[at] = (normalized(cell) * head_gain).astype(bf16)
            if b < 3:
                block = (memories[n * 128 : n * 128 + 128, :], peak[n : n + 1, :] * ones, total[n : n + 1, :] * ones)
                state = merged(state, block)
    count = own.shape[0]
    rank = place[0]
    for target, device, start in (
        (own, rank, 0),
        (near, rank ^ 1, 0),
        (far, 3 - rank, 0),
        (across_near, rank ^ 2, 0),
        (across_far, rank ^ 2, count // 2),
    ):
        at = pl.ds(pl.multiple_of(device * count + start, count // 2), target.shape[0])
        target[...] = jnp.dot(cells[at, :], weight[...], preferred_element_type=f32).astype(bf16)


def relay_kernel(near, far, from_near, from_far, to_near, to_far):
    half = from_near.shape[0]
    to_far[:half, :] = (far[:half, :].astype(f32) + from_near[...].astype(f32)).astype(bf16)
    to_far[half:, :] = far[half:, :]
    to_near[:half, :] = near[:half, :]
    to_near[half:, :] = (near[half:, :].astype(f32) + from_far[...].astype(f32)).astype(bf16)


def sum_kernel(own, near, far, out):
    total = own[...].astype(f32) + near[...].astype(f32) + far[...].astype(f32)
    out[...] = total.astype(bf16)


def cut_kernel(place, weights, far_weights, keep, give):
    rank = place[0]
    units = weights.shape[0]
    share = weights.shape[1] // 4
    for target, device in ((keep, rank), (give, rank ^ 1)):
        for j, quarter in enumerate((device, 3 - device)):
            at = pl.ds(pl.multiple_of(quarter * share, share), share)
            columns = slice(j * share, (j + 1) * share)
            target[:units, columns] = weights[:, at]
            target[units:, columns] = far_weights[:, at]


def started(copies):
    for copy in copies:
        copy.start()
    return copies


def dispatch_kernel(
    place, rows, gain_in, group_in, expert_in, routes, send_out, notes_out,
    gain, group_router, expert_router, normed, send, notes, sems,
):
    rank, core = place[0], place[1]
    sources = ((gain_in, gain), (group_in, group_router), (expert_in, expert_router))
    copies = started([pltpu.make_async_copy(a, b, sems.at[n]) for n, (a, b) in enumerate(sources)])
    for copy in copies:
        copy.wait()
    normed[...] = (normalized(rows[...].astype(f32)) * gain[...]).astype(bf16)

    def logits(weights):
        return lax.dot_general(
            weights[...], normed[...], (((1,), (1,)), ((), ())), preferred_element_type=f32
        )

    group_logits, expert_logits = logits(group_router), logits(expert_router)
    experts, tokens = expert_logits.shape
    groups = group_logits.shape[0]
    expert_ids = lax.broadcasted_iota(jnp.int32, (experts, tokens), 0)
    group_ids = lax.broadcasted_iota(jnp.int32, (groups, tokens), 0)
    named = [routes[k : k + 1, :] for k in range(2)]
    hot = [(expert_ids == e).astype(f32) for e in named]
    above = (
        lax.broadcasted_iota(jnp.int32, (tokens, tokens), 0)
        < lax.broadcasted_iota(jnp.int32, (tokens, tokens), 1)
    ).astype(bf16)
    counts = [jnp.dot(h.astype(bf16), above, preferred_element_type=f32) for h in hot]
    counts[1] = counts[1] + jnp.sum(hot[0], axis=1, keepdims=True)
    slots = []
    for k in range(2):
        at = jnp.sum(hot[k] * counts[k], axis=0, keepdims=True).astype(jnp.int32)
        slots.append(jnp.where((named[k] & 1) == core, (named[k] >> 1) * 16 + at, -1))
    chosen = [jnp.sum(h * expert_logits, axis=0, keepdims=True) for h in hot]
    grouped = [
        jnp.sum(jnp.where(group_ids == e // (experts // groups), group_logits, 0.0), axis=0, keepdims=True)
        for e in named
    ]
    combine = [
        jax.nn.sigmoid(grouped[k]) * jax.nn.sigmoid(chosen[k] - chosen[1 - k]) for k in range(2)
    ]
    share = rows.shape[1] // 4
    row = lax.broadcasted_iota(jnp.int32, (128, tokens), 0)
    wide = jnp.where(row == 0, slots[0].astype(f32), slots[1].astype(f32))
    notes[...] = jnp.where(row < 2, wide, jnp.where(row == 2, combine[0], combine[1])).T
    copies = started([pltpu.make_async_copy(notes, notes_out, sems.at[0])])
    half = send.shape[0] // 2
    slot_ids = lax.broadcasted_iota(jnp.int32, (half, tokens), 0)
    for n in range(2):
        at = pl.ds(n * half, half)
        ids = slot_ids + n * half
        pick = ((ids == slots[0]) | (ids == slots[1])).astype(bf16)
        for j, quarter in enumerate((rank, 3 - rank)):
            features = normed[:, pl.ds(pl.multiple_of(quarter * share, share), share)]
            send[at, j * share : (j + 1) * share] = jnp.dot(
                pick, features, preferred_element_type=f32
            ).astype(bf16)
        copies += started([pltpu.make_async_copy(send.at[at], send_out.at[at], sems.at[n + 1])])
    for copy in copies:
        copy.wait()


def hidden_kernel(
    place, own, other, gate_in, up_in, far_gate_in, far_up_in, out,
    rows, gate, up, far_gate, far_up, sems,
):
    rank = place[0]
    share = own.shape[1] // 2
    units = gate.shape[1]
    copies = []
    for source, device in ((own, rank), (other, rank ^ 1)):
        for j, quarter in enumerate((device, 3 - device)):
            at = pl.ds(pl.multiple_of(quarter * share, share), share)
            copies.append((source.at[:, j * share : (j + 1) * share], rows.at[:, at]))
    copies += [(gate_in, gate), (up_in, up), (far_gate_in, far_gate), (far_up_in, far_up)]
    copies = started([pltpu.make_async_copy(a, b, sems.at[n]) for n, (a, b) in enumerate(copies)])
    for copy in copies[:5]:
        copy.wait()
    for part, (g, u) in enumerate(((gate, up), (far_gate, far_up))):
        if part == 1:
            copies[6].wait()
        gate_act = jnp.dot(rows[...], g[...], preferred_element_type=f32)
        copies[5 + 2 * part].wait()
        up_act = jnp.dot(rows[...], u[...], preferred_element_type=f32)
        out[:, part * units : (part + 1) * units] = (jax.nn.silu(gate_act) * up_act).astype(bf16)


def down_kernel(own, other, mine_in, theirs_in, out, mine, theirs, sems):
    copies = started(
        [
            pltpu.make_async_copy(mine_in, mine, sems.at[0]),
            pltpu.make_async_copy(theirs_in, theirs, sems.at[1]),
        ]
    )
    copies[0].wait()
    total = jnp.dot(own[...], mine[...], preferred_element_type=f32)
    copies[1].wait()
    total = total + jnp.dot(other[...], theirs[...], preferred_element_type=f32)
    out[...] = total.astype(bf16)


def combine_kernel(notes, rows, keep, send):
    tokens, share = keep.shape
    slots = [notes[:, k : k + 1].astype(jnp.int32) for k in range(2)]
    lanes = lax.broadcasted_iota(jnp.int32, (tokens, rows.shape[0]), 1)
    weight = jnp.where(lanes == slots[0], notes[:, 2:3], 0.0) + jnp.where(
        lanes == slots[1], notes[:, 3:4], 0.0
    )
    high = weight.astype(bf16)
    low = (weight - high.astype(f32)).astype(bf16)
    total = jnp.dot(high, rows[...], preferred_element_type=f32)
    total = total + jnp.dot(low, rows[...], preferred_element_type=f32)
    keep[...] = total[:, :share]
    send[...] = total[:, share:].astype(bf16)


def last_kernel(first, second, out):
    out[...] = (first[...] + second[...].astype(f32)).astype(bf16)


def run(
    kernel, shapes, args, place=None, scratch=(), room=8,
    hbm_in=(), hbm_out=(), sems=0, free_in=(), free_out=(),
):
    def block(shape):
        return pl.BlockSpec(tuple(shape), lambda n: (0,) * len(shape))

    far = pl.BlockSpec(memory_space=pltpu.HBM)
    near = pl.BlockSpec(memory_space=pltpu.VMEM)

    def spec(n, shape, copied, free):
        return far if n in copied else near if n in free else block(shape)

    specs = [spec(n, a.shape, hbm_in, free_in) for n, a in enumerate(args)]
    args = [
        a if n in free_in else pltpu.with_memory_space_constraint(a, pltpu.HBM)
        for n, a in enumerate(args)
    ]
    if place is not None:
        specs = [pl.BlockSpec(memory_space=pltpu.SMEM)] + specs
        args = (place, *args)
    outs = tuple(
        jax.ShapeDtypeStruct(s, d) if n in free_out else pltpu.HBM(s, d) for n, (s, d) in enumerate(shapes)
    )
    scratch = [pltpu.VMEM(s, d) for s, d in scratch]
    if sems:
        scratch.append(pltpu.SemaphoreType.DMA((sems,)))
    result = pl.pallas_call(
        kernel,
        out_shape=outs,
        grid=(1,),
        in_specs=specs,
        out_specs=tuple(spec(n, o.shape, hbm_out, free_out) for n, o in enumerate(outs)),
        scratch_shapes=scratch,
        compiler_params=pltpu.CompilerParams(vmem_limit_bytes=room * 1024 * 1024),
    )(*args)
    return result if len(outs) > 1 else result[0]


def traded(x, axis):
    return lax.all_to_all(x, axis, 0, 0, tiled=True)


def shards(
    mixer_in,
    mixer_gain,
    query_weight,
    key_weight,
    value_weight,
    input_gate,
    forget_gate,
    head_gain,
    mixer_out_weight,
    expert_in,
    expert_gain,
    group_router,
    expert_router,
    routes,
    gate_experts,
    up_experts,
    down_experts,
):
    place = jnp.stack([lax.axis_index(a) for a in ("tp", "c", "z", "y")]).astype(jnp.int32)
    tokens, width = expert_in.shape
    share = width // 4
    slots = 32 * 16
    gate, up, down = gate_experts[0], up_experts[0], down_experts[0]
    units = gate.shape[1]
    held_rows = lax.ppermute(expert_in, ("c", "tp"), CROSS)
    held_routes = lax.ppermute(routes.T, ("c", "tp"), CROSS)
    far_down = lax.ppermute(down, "tp", FAR)
    far_gate = lax.ppermute(gate, "tp", FAR)
    far_up = lax.ppermute(up, "tp", FAR)
    groups, experts = group_router.shape[1], expert_router.shape[1]
    send, notes = run(
        dispatch_kernel,
        (((slots, 2 * share), bf16), ((tokens, 128), f32)),
        (held_rows, expert_gain.reshape(1, -1), group_router.T, expert_router.T, held_routes),
        place,
        [
            ((1, width), f32),
            ((groups, width), bf16),
            ((experts, width), bf16),
            ((tokens, width), bf16),
            ((slots, 2 * share), bf16),
            ((tokens, 128), f32),
        ],
        room=16,
        hbm_in=(1, 2, 3),
        hbm_out=(0, 1),
        sems=3,
        free_in=(0, 4),
    )
    arrived = traded(send, ZY)

    down_mine, give = run(
        cut_kernel, (((2 * units, 2 * share), bf16),) * 2, (down, far_down), place, room=16, free_in=(1,)
    )
    down_theirs = lax.ppermute(give, "tp", NEAR)

    row_count = mixer_in.shape[0]
    local = query_weight.shape[1]
    log_forget = jax.nn.log_sigmoid(forget_gate).reshape(8, 128)
    inputs = input_gate.reshape(8, 128)
    q, k, v, memories, spread = run(
        mixer_head_kernel,
        (((row_count, local), bf16),) * 3 + (((8 * 128, 128), f32), ((8 * LINES, 128), f32)),
        (mixer_in, mixer_gain.reshape(1, -1), query_weight, key_weight, value_weight, log_forget, inputs),
        None,
        [((row_count, width), bf16)],
        room=24,
    )
    members = traded(spread, YC)
    spread, before = run(
        fold_slab_kernel, (((8 * LINES, 128), f32), ((2 * LINES, 128), f32)), (members,), place, free_in=(0,)
    )
    slabs = traded(spread, "z")
    mine, theirs = run(
        fold_all_kernel, (((LINES, 128), f32),) * 2, (slabs, before), place, free_in=(0,), free_out=(0, 1)
    )
    theirs = lax.ppermute(theirs, "c", SWAP)
    count = row_count // 4
    own, near, far, across_near, across_far = run(
        mixer_tail_kernel,
        (((count, width), bf16),) * 3 + (((count // 2, width), bf16),) * 2,
        (q, k, v, log_forget, inputs, memories, mine, theirs, head_gain.reshape(1, -1), mixer_out_weight),
        place,
        [((row_count, local), bf16)],
        room=16,
        free_in=(6, 7),
        free_out=(3, 4),
    )
    from_near = lax.ppermute(across_near, "tp", NEAR)
    from_far = lax.ppermute(across_far, "tp", FAR)
    to_near, to_far = run(
        relay_kernel, (((count, width), bf16),) * 2, (near, far, from_near, from_far), free_in=(2, 3), free_out=(0, 1)
    )
    near = lax.ppermute(to_near, "tp", NEAR)
    far = lax.ppermute(to_far, "tp", FAR)
    mixer_out = run(sum_kernel, (((count, width), bf16),), (own, near, far), free_in=(1, 2))

    other_rows = lax.ppermute(arrived, "tp", NEAR)
    hidden = run(
        hidden_kernel,
        (((slots, 2 * units), bf16),),
        (arrived, other_rows, gate, up, far_gate, far_up),
        place,
        [((slots, width), bf16)] + [((width, units), bf16)] * 4,
        room=16,
        hbm_in=range(6),
        sems=8,
        free_out=(0,),
    )
    other_hidden = lax.ppermute(hidden, "tp", NEAR)
    result = run(
        down_kernel,
        (((slots, 2 * share), bf16),),
        (hidden, other_hidden, down_mine, down_theirs),
        None,
        [((2 * units, 2 * share), bf16)] * 2,
        room=16,
        hbm_in=(2, 3),
        sems=2,
        free_in=(0, 1),
    )
    back = traded(result, ZY)
    keep, give = run(
        combine_kernel, (((tokens, share), f32), ((tokens, share), bf16)), (notes, back), free_in=(1,), free_out=(0, 1)
    )
    kept = lax.ppermute(keep, ("c", "tp"), CROSS)
    received = lax.ppermute(give, ("c", "tp"), LAST)
    expert_out = run(last_kernel, (((tokens, share), bf16),), (kept, received), free_in=(0, 1))
    return (mixer_out, expert_out)


def solution(mesh):
    split = Mesh(mesh.devices.reshape(8, 4, 2, mesh.shape["tp"]), EP_TP)
    placed = (
        P(EP, None),
        P(),
        P(None, "tp"),
        P(None, "tp"),
        P(None, "tp"),
        P("tp", EP),
        P("tp", EP),
        P(),
        P("tp", None),
        P(EP, None),
        P(),
        P(),
        P(),
        P(EP, None),
        P(EP, None, "tp"),
        P(EP, None, "tp"),
        P(EP, "tp", None),
    )

    return jax.shard_map(
        shards,
        mesh=split,
        in_specs=placed,
        out_specs=(P(EP_TP, None), P(EP, "tp")),
        check_vma=False,
    )
```
